768 devices in a mesh: ep: 24 (over z, core), tp: 32 (over y, x).
Axes of the slice: x: 4, y: 8, z: 12, core: 2. Of those that a mesh axis runs over, the one named last changes fastest.
Arguments:
- tokens: bfloat16 [3072, 2048], P('ep', 'tp'), may hold values from -6 to 6
- routes: int32 [3072, 2], P('ep'), may hold values from 0 to 23, as said below
- route_weights: float32 [3072, 2], P('ep'), may hold values from 0.1 to 1
- grad_out: bfloat16 [3072, 2048], P('ep', 'tp'), may hold values from -6 to 6
- w_gate: bfloat16 [24, 2048, 2048], P('ep', 'tp'), may hold values from -0.125 to 0.125
- w_up: bfloat16 [24, 2048, 2048], P('ep', 'tp'), may hold values from -0.125 to 0.125
- w_down: bfloat16 [24, 2048, 2048], P('ep', 'tp')
Outputs:
- grad_tokens: bfloat16 [3072, 2048], P('ep', 'tp')
- grad_route: float32 [3072, 2], P('ep')
- grad_gate: float32 [24, 2048, 2048], P('ep', 'tp')
- grad_up: float32 [24, 2048, 2048], P('ep', 'tp')
- grad_down: float32 [24, 2048, 2048], P('ep', 'tp')
- gate_row_norms: float32 [24, 2048], P('ep')
- up_row_norms: float32 [24, 2048], P('ep')
- down_row_norms: float32 [24, 2048], P('ep', 'tp')
The draws below stay inside these ranges and needn't reach their ends.
Inputs may be any that keep to these rules, and one draw needn't show every extreme that they name: `routes`: each token names two different experts of one group: group g holds experts g * 4 to g * 4 + 3. Among the 128 rows of one device along ep no expert is named more than 16 times, and in every draw some expert is named exactly 16 times by the rows of every device along ep.
All inputs are finite; a program needn't handle non-finite values.
Results may differ from the reference program's by a relative error of at most 0.017.
Values may be sent and summed in bfloat16 or wider, within the bound.
No kernel may reach another device: no remote copies, remote signals or barrier semaphores. Data moves between devices by JAX's collectives and lax.ppermute only.
A program may use at most 64 MiB of HBM per device.

```python
import jax
import jax.numpy as jnp
from jax import lax

D = 2048
FF = 2048
TOP = 2
GROUP_SIZE = 4
TOK_DEV = 128
EXPERTS = 24
TOKENS = 3072
CAP = 16
N_EP = 24
N_TP = 32


def permute_four(sub_key):
    return jax.random.permutation(sub_key, GROUP_SIZE)


def draw_routes(key, part):
    group_total = EXPERTS // GROUP_SIZE
    hot_group = jax.random.randint(jax.random.fold_in(key, 11), (), 0, group_total)
    hot_count = 2 * CAP
    remaining = TOK_DEV - hot_count
    if group_total > 1:
        even_share = remaining // (group_total - 1)
        leftover = remaining % (group_total - 1)
        other_counts = even_share + (jnp.arange(group_total - 1) < leftover).astype(jnp.int32)
        by_rank = jnp.concatenate([jnp.array([hot_count], jnp.int32), other_counts.astype(jnp.int32)])
    else:
        by_rank = jnp.array([hot_count], jnp.int32)
    pair_table = jnp.array([[0, 1], [2, 3], [0, 2], [1, 3], [0, 3], [1, 2]], jnp.int32)

    def one_block(block_key):
        sub_keys = jax.random.split(block_key, 4)
        group_order = jax.random.permutation(sub_keys[0], group_total)
        first_group = group_order[0]
        group_order = jnp.where(group_order == hot_group, first_group, group_order)
        group_order = group_order.at[0].set(hot_group)
        group_counts = jnp.zeros((group_total,), jnp.int32).at[group_order].set(by_rank)
        group_ends = jnp.cumsum(group_counts)
        group_starts = group_ends - group_counts
        positions = jnp.arange(TOK_DEV, dtype=jnp.int32)
        group_of = jnp.sum((positions[:, None] >= group_ends[None, :]).astype(jnp.int32), axis=1)
        within = positions - group_starts[group_of]
        pair_rows = pair_table[within % 6]
        inner_perm = jax.vmap(permute_four)(jax.random.split(sub_keys[1], group_total))
        chosen = jnp.take_along_axis(inner_perm[group_of], pair_rows, axis=1)
        swap_bit = jax.random.randint(sub_keys[2], (TOK_DEV, 1), 0, 2)
        chosen = jnp.where(swap_bit == 1, chosen[:, ::-1], chosen)
        expert_ids = group_of[:, None] * GROUP_SIZE + chosen
        shuffle = jax.random.permutation(sub_keys[3], TOK_DEV)
        return expert_ids[shuffle]
    all_blocks = jax.vmap(one_block)(jax.random.split(jax.random.fold_in(key, 12), N_EP))
    return all_blocks.reshape(TOKENS, 2).astype(jnp.int32)


def draw_w_down(key, part):
    noise = jnp.clip(jax.random.normal(jax.random.fold_in(key, 21), (EXPERTS, FF, D), jnp.float32), -6.0, 6.0)
    ramp = 3.0 ** (jnp.arange(FF, dtype=jnp.float32) / FF)
    jitter = jnp.exp(jax.random.uniform(jax.random.fold_in(key, 23), (EXPERTS, FF, 1), jnp.float32, -0.7, 0.7))
    row_scale = ramp[None, :, None] * jitter / jnp.sqrt(jnp.mean(ramp * ramp))
    return (noise * row_scale * FF ** (-0.5)).astype(jnp.bfloat16)


def block_levels(rng, extent, cuts, low, top_value):
    def one(axis_at, shards_of):
        draws = jax.random.uniform(jax.random.fold_in(jax.random.fold_in(rng, 6), axis_at), (shards_of,), jnp.float32, low / len(cuts), top_value / len(cuts))
        return jnp.repeat(jnp.exp(draws), extent[axis_at] // shards_of).reshape((-1,) + (1,) * (len(extent) - axis_at - 1))

    level = one(*cuts[0])
    for cut in cuts[1:]:
        level = level * one(*cut)
    return level


def normal_values(own_key, shape, scale, reach, cuts=(), held_as=jnp.bfloat16):
    result = jax.random.normal(own_key, shape, jnp.float32) * scale
    if len(cuts) > 0:
        result = block_levels(own_key, shape, cuts, -0.22, 0.18) * result
    return jnp.clip(result, min=-reach, max=reach).astype(held_as)


def setup_inputs(seed: int = 0) -> dict:
    key_list = jax.random.split(jax.random.key(seed), 8)
    tokens = normal_values(key_list[0], (TOKENS, D), 1.0, 6.0, ((0, 24), (1, 32)))
    routes = draw_routes(jax.random.fold_in(key_list[7], 71), 0)
    route_weights = jnp.clip(0.1 + 0.9 * jax.random.uniform(key_list[2], (TOKENS, TOP), jnp.float32) ** block_levels(key_list[2], (TOKENS, TOP), ((0, 24),), -0.2, 0.2), 0.1, 1.0)
    grad_out = normal_values(key_list[3], (TOKENS, D), 1.0, 6.0, ((0, 24), (1, 32)))
    w_gate = normal_values(key_list[4], (EXPERTS, FF, D), D ** -0.5, 0.125, ((0, 24), (1, 32)))
    w_up = normal_values(key_list[5], (EXPERTS, FF, D), D ** -0.5, 0.125, ((0, 24), (1, 32)))
    w_down = draw_w_down(jax.random.fold_in(key_list[7], 71), 0)
    return {"tokens": tokens, "routes": routes, "route_weights": route_weights, "grad_out": grad_out, "w_gate": w_gate, "w_up": w_up, "w_down": w_down}


def silu_parts(pre_act):
    sigmoid_val = jax.nn.sigmoid(pre_act)
    return pre_act * sigmoid_val, sigmoid_val * (1.0 + pre_act * (1.0 - sigmoid_val))


def reference(tokens, routes, route_weights, grad_out, w_gate, w_up, w_down):
    token_total, model_width = tokens.shape
    hidden_width = w_gate.shape[1]
    flat_ids = routes.reshape(-1).astype(jnp.int32)
    slot_total = flat_ids.shape[0]
    one_hot = (flat_ids[:, None] == jnp.arange(EXPERTS, dtype=jnp.int32)[None, :]).astype(jnp.int32)
    blocked = one_hot.reshape(N_EP, slot_total // N_EP, EXPERTS)
    earlier = jnp.cumsum(blocked, axis=1) - blocked
    slot_ids = jnp.sum(earlier * blocked, axis=2).reshape(-1).astype(jnp.int32)
    source = (jnp.arange(slot_total, dtype=jnp.int32) // (slot_total // N_EP)).astype(jnp.int32)
    position = (source * CAP + slot_ids).astype(jnp.int32)
    index_table = jnp.full((EXPERTS, N_EP * CAP), slot_total, jnp.int32)
    index_table = index_table.at[flat_ids, position].set(jnp.arange(slot_total, dtype=jnp.int32))
    weight_flat = route_weights.reshape(-1)
    zero_row = jnp.zeros((1, model_width), jnp.bfloat16)
    token_rows = jnp.concatenate([jnp.repeat(tokens, 2, axis=0), zero_row], axis=0)
    scaled = (weight_flat[:, None] * jnp.repeat(grad_out, 2, axis=0).astype(jnp.float32)).astype(jnp.bfloat16)
    scaled_rows = jnp.concatenate([scaled, zero_row], axis=0)
    block_width = hidden_width // N_TP

    def one_expert(item):
        indices, gate_w, up_w, down_w = item
        x_rows = token_rows[indices]
        s_rows = scaled_rows[indices]
        gate = jnp.dot(x_rows, gate_w.T, preferred_element_type=jnp.float32)
        up = jnp.dot(x_rows, up_w.T, preferred_element_type=jnp.float32)
        active, slope = silu_parts(gate)
        hidden = (active * up).astype(jnp.bfloat16)
        dhid = jnp.dot(s_rows, down_w.T, preferred_element_type=jnp.float32)
        partial_value = jnp.sum(hidden.astype(jnp.float32) * dhid, axis=1)
        dgate = (dhid * up * slope).astype(jnp.bfloat16)
        dup = (dhid * active).astype(jnp.bfloat16)
        gate_grad = jnp.dot(dgate.T, x_rows, preferred_element_type=jnp.float32)
        up_grad = jnp.dot(dup.T, x_rows, preferred_element_type=jnp.float32)
        down_grad = jnp.dot(hidden.T, s_rows, preferred_element_type=jnp.float32)
        row_count = x_rows.shape[0]
        dgate_blocks = dgate.astype(jnp.float32).reshape(row_count, N_TP, block_width)
        dup_blocks = dup.astype(jnp.float32).reshape(row_count, N_TP, block_width)
        gate_blocks = gate_w.astype(jnp.float32).reshape(N_TP, block_width, model_width)
        up_blocks = up_w.astype(jnp.float32).reshape(N_TP, block_width, model_width)
        pieces = jnp.einsum('rjf,jfd->jrd', dgate_blocks, gate_blocks) + jnp.einsum('rjf,jfd->jrd', dup_blocks, up_blocks)
        rounded = lax.optimization_barrier(pieces.astype(jnp.bfloat16))
        dtok = jnp.sum(rounded.astype(jnp.float32), axis=0)
        return dtok, partial_value, gate_grad, up_grad, down_grad

    dtok_all, partial_all, grad_gate, grad_up, grad_down = lax.map(one_expert, (index_table, w_gate, w_up, w_down))
    dtok_slots = dtok_all[flat_ids, position]
    grad_tokens = jnp.sum(dtok_slots.reshape(token_total, 2, model_width), axis=1).astype(jnp.bfloat16)
    grad_route = (partial_all[flat_ids, position] / weight_flat).reshape(token_total, 2)
    gate_row_norms = jnp.sum(grad_gate * grad_gate, axis=1)
    up_row_norms = jnp.sum(grad_up * grad_up, axis=1)
    down_row_norms = jnp.sum(grad_down * grad_down, axis=2)
    return (grad_tokens, grad_route, grad_gate, grad_up, grad_down, gate_row_norms, up_row_norms, down_row_norms)
```

```python
import jax
import jax.numpy as jnp
from jax import lax
from jax.experimental import pallas as pl
from jax.sharding import Mesh
from jax.sharding import PartitionSpec as P


SLOTS = 16
HALF = 64
F32 = jnp.float32
BF16 = jnp.bfloat16


def dot(a, b, ca, cb):
    return lax.dot_general(a, b, (((ca,), (cb,)), ((), ())), preferred_element_type=F32)


def split_hi_lo(v):
    hi = v.astype(BF16)
    return hi, (v - hi.astype(F32)).astype(BF16)


def placed(routes, tokens, experts):
    ids = lax.broadcasted_iota(jnp.int32, (experts, tokens), 0)
    first = ids == routes[0:1, :]
    second = ids == routes[1:2, :]
    named = (first | second).astype(F32).astype(BF16)
    before = (
        lax.broadcasted_iota(jnp.int32, (tokens, tokens), 0)
        < lax.broadcasted_iota(jnp.int32, (tokens, tokens), 1)
    ).astype(F32).astype(BF16)
    rank = dot(named, before, 1, 0) + (ids * SLOTS).astype(F32)
    return [
        jnp.sum(jnp.where(m, rank, 0.0), axis=0, keepdims=True).astype(jnp.int32)
        for m in (first, second)
    ]


def chosen(position, slots):
    at = lax.broadcasted_iota(jnp.int32, (slots, position.shape[1]), 0)
    return (at == position).astype(F32).astype(BF16)


def dispatch_body(tokens, routes, weights, cotangent, sent, positions):
    width, count = tokens.shape
    slots = sent.shape[0]
    at = placed(routes[...], count, slots // SLOTS)
    positions[...] = jnp.concatenate(at, axis=0)
    x = tokens[...]
    g = cotangent[...].astype(F32)
    scaled = [(g * weights[k : k + 1, :]).astype(BF16) for k in range(2)]
    rows = jnp.concatenate(
        [jnp.concatenate([x, x], axis=1), jnp.concatenate(scaled, axis=1)], axis=0
    )
    pick = jnp.concatenate([chosen(p, slots) for p in at], axis=1)
    sent[...] = dot(pick, rows, 1, 1).astype(BF16)


def quarter_weights_body(w_gate, w_up, w_down, out):
    nx = out.shape[0]
    hid = w_gate.shape[0]
    for m, w in enumerate((w_gate, w_up, w_down)):
        for q in range(nx):
            for j in range(out.shape[2] // 128):
                a, b = ((2 * j) * nx + q) * HALF, ((2 * j + 1) * nx + q) * HALF
                out[q, m * hid : (m + 1) * hid, j * 128 : (j + 1) * 128] = jnp.concatenate(
                    [w[:, a : a + HALF], w[:, b : b + HALF]], axis=1
                )


def partial_body(rows, weights, out, x_out, s_out):
    ny = rows.shape[0]
    for j in range(ny // 2):
        a, b = rows[2 * j], rows[2 * j + 1]
        x_out[:, j * 128 : (j + 1) * 128] = jnp.concatenate([a[:, :HALF], b[:, :HALF]], axis=1)
        s_out[:, j * 128 : (j + 1) * 128] = jnp.concatenate([a[:, HALF:], b[:, HALF:]], axis=1)
    x, s = x_out[...], s_out[...]
    hid = weights.shape[1] // 3
    for q in range(weights.shape[0]):
        out[q, : 2 * hid, :] = dot(weights[q, : 2 * hid, :], x, 1, 1).astype(BF16)
        out[q, 2 * hid :, :] = dot(weights[q, 2 * hid :, :], s, 1, 1).astype(BF16)


def activation_body(parts, out):
    total = parts[0].astype(F32)
    for q in range(1, parts.shape[0]):
        total = total + parts[q].astype(F32)
    hid = total.shape[0] // 3
    gate, up, dhid = total[:hid], total[hid : 2 * hid], total[2 * hid :]
    sig = 1.0 / (1.0 + jnp.exp(-gate))
    active = gate * sig
    slope = sig * (1.0 + gate * (1.0 - sig))
    hidden = (active * up).astype(BF16)
    dgate = (dhid * up * slope).astype(BF16)
    dup = (dhid * active).astype(BF16)
    value = jnp.sum(hidden.astype(F32) * dhid, axis=0, keepdims=True)
    hi, lo = split_hi_lo(value)
    pad = jnp.zeros((out.shape[1] - 3 * hid - 2, out.shape[2]), BF16)
    block = jnp.concatenate([dgate, dup, hidden, hi, lo, pad], axis=0)
    for q in range(out.shape[0]):
        out[q] = block


def backward_body(acts, weights, x_rows, s_rows, back, grads):
    nx, ny = acts.shape[0], back.shape[0]
    hid = weights.shape[1] // 3
    width = weights.shape[2]
    slots = acts.shape[2]
    terms = dot(weights[0, : 2 * hid, :], acts[0, : 2 * hid, :], 0, 0)
    for q in range(1, nx):
        terms = terms + dot(weights[q, : 2 * hid, :], acts[q, : 2 * hid, :], 0, 0)
    terms = terms.astype(BF16)
    x, s = x_rows[...], s_rows[...]
    norms = [jnp.zeros((1, width), F32) for _ in range(2)]
    value = jnp.zeros((1, slots), F32)
    for q in range(nx):
        pair = dot(acts[q, : 2 * hid, :], x, 1, 0)
        down = dot(acts[q, 2 * hid : 3 * hid, :], s, 1, 0)
        grads[q, : 2 * hid, :] = pair.astype(BF16)
        grads[q, 2 * hid :, :] = down.astype(BF16)
        for m in range(2):
            part = pair[m * hid : (m + 1) * hid]
            norms[m] = norms[m] + jnp.sum(part * part, axis=0, keepdims=True)
        tail = acts[q, 3 * hid : 3 * hid + 2, :].astype(F32)
        value = value + tail[0:1] + tail[1:2]
    lines = list(split_hi_lo(value))
    rest = jnp.zeros((1, 2 * slots - width), BF16)
    for n in norms:
        for v in split_hi_lo(n):
            lines += [v[:, :slots], jnp.concatenate([v[:, slots:], rest], axis=1)]
    pad = jnp.zeros((back.shape[1] - HALF - len(lines), slots), BF16)
    extra = jnp.concatenate(lines + [pad], axis=0)
    for j in range(ny):
        back[j, :HALF, :] = terms[j * HALF : (j + 1) * HALF]
        back[j, HALF:, :] = extra


def gathered_body(parts, sent, norms):
    total = parts[0].astype(F32)
    for j in range(1, parts.shape[0]):
        total = total + parts[j].astype(F32)
    slots = total.shape[1]
    hi, lo = split_hi_lo(total[HALF : HALF + 1] + total[HALF + 1 : HALF + 2])
    pad = jnp.zeros((128 - HALF - 2, slots), F32)
    block = jnp.concatenate([total[:HALF], hi.astype(F32), lo.astype(F32), pad], axis=0)
    sent[...] = block.T.astype(BF16)
    tail = total[HALF + 2 : HALF + 10]
    lines = []
    for m in range(2):
        one = tail[4 * m : 4 * m + 2] + tail[4 * m + 2 : 4 * m + 4]
        lines += [one[0:1, c * 128 : (c + 1) * 128] for c in range(slots // 128)]
        lines += [one[1:2, 0:128]]
    norms[...] = jnp.concatenate(lines, axis=0)


def combine_body(back, positions, weights, grad_tokens, grad_route):
    slots, count = back.shape[0], positions.shape[1]
    pick = jnp.concatenate([chosen(positions[k : k + 1, :], slots) for k in range(2)], axis=1)
    got = dot(back[...], pick, 0, 0)
    grad_tokens[...] = (got[:HALF, :count] + got[:HALF, count:]).astype(BF16)
    value = got[HALF : HALF + 1] + got[HALF + 1 : HALF + 2]
    value = jnp.concatenate([value[:, :count], value[:, count:]], axis=0)
    grad_route[...] = value / weights[...]


def grads_body(parts, grad_gate, grad_up, grad_down, down_norms):
    nx = parts.shape[0]
    hid = grad_gate.shape[0]
    ny = parts.shape[2] // HALF
    acc = jnp.zeros((hid, 128), F32)
    for m, out in enumerate((grad_gate, grad_up, grad_down)):
        for y in range(ny):
            for h in range(nx // 2):
                tile = jnp.concatenate(
                    [
                        parts[2 * h, m * hid : (m + 1) * hid, y * HALF : (y + 1) * HALF],
                        parts[2 * h + 1, m * hid : (m + 1) * hid, y * HALF : (y + 1) * HALF],
                    ],
                    axis=1,
                ).astype(F32)
                at = (y * (nx // 2) + h) * 128
                out[:, at : at + 128] = tile
                if m == 2:
                    acc = acc + tile * tile
    down_norms[...] = jnp.sum(acc.T, axis=0, keepdims=True)


def norms_body(parts, gate_norms, up_norms):
    nx = parts.shape[0]
    for m, out in enumerate((gate_norms, up_norms)):
        lines = []
        for y in range(8):
            half = (y % 2) * HALF
            for h in range(nx // 2):
                row = m * 4 + y // 2
                lines.append(
                    jnp.concatenate(
                        [
                            parts[2 * h, row : row + 1, half : half + HALF],
                            parts[2 * h + 1, row : row + 1, half : half + HALF],
                        ],
                        axis=1,
                    )
                )
        out[...] = jnp.concatenate(lines, axis=0)


def call(body, outs, *args, name):
    return pl.pallas_call(
        body,
        out_shape=[jax.ShapeDtypeStruct(s, d) for s, d in outs],
        name=name,
    )(*args)


def swap(a, axis):
    return lax.all_to_all(a, axis, 0, 0, tiled=True)


def per_device(tokens, routes, route_weights, grad_out, w_gate, w_up, w_down):
    ny, nx = lax.axis_size("y"), lax.axis_size("x")
    sources = lax.axis_size("z") * lax.axis_size("c")
    count, feat = tokens.shape
    _, hid, width = w_gate.shape
    slots = sources * SLOTS
    quarter = width // nx
    sent, positions = call(
        dispatch_body,
        [((slots, 2 * feat), BF16), ((2, count), jnp.int32)],
        tokens.T,
        routes.T,
        route_weights.T,
        grad_out.T,
        name="dispatch",
    )
    (w_sent,) = call(
        quarter_weights_body,
        [((nx, 3 * hid, quarter), BF16)],
        w_gate[0],
        w_up[0],
        w_down[0],
        name="quarter_weights",
    )
    weights = swap(w_sent, "x")
    mine = swap(sent.reshape(sources, SLOTS, 2 * feat), ("z", "c")).reshape(slots, 2 * feat)
    rows = lax.all_gather(mine, "y", axis=0, tiled=False)
    parts, x_rows, s_rows = call(
        partial_body,
        [
            ((nx, 3 * hid, slots), BF16),
            ((slots, quarter), BF16),
            ((slots, quarter), BF16),
        ],
        rows,
        weights,
        name="partial",
    )
    parts = swap(parts, "x")
    (acts,) = call(activation_body, [((nx, 3 * hid + 16, slots), BF16)], parts, name="activation")
    acts = swap(acts, "x")
    back, grads = call(
        backward_body,
        [((ny, feat + 16, slots), BF16), ((nx, 3 * hid, quarter), BF16)],
        acts,
        weights,
        x_rows,
        s_rows,
        name="backward",
    )
    back = swap(back, "y")
    grads = swap(grads, "x")
    back_sent, norms = call(
        gathered_body,
        [((slots, 128), BF16), ((8, 128), F32)],
        back,
        name="gathered",
    )
    norms = lax.all_gather(norms, "x", axis=0, tiled=False)
    back = swap(back_sent.reshape(sources, SLOTS, 128), ("z", "c")).reshape(slots, 128)
    grad_tokens, grad_route = call(
        combine_body,
        [((feat, count), BF16), ((2, count), F32)],
        back,
        positions,
        route_weights.T,
        name="combine",
    )
    grad_gate, grad_up, grad_down, down_norms = call(
        grads_body,
        [((hid, width), F32)] * 3 + [((1, hid), F32)],
        grads,
        name="grads",
    )
    gate_norms, up_norms = call(
        norms_body, [((width // 128, 128), F32)] * 2, norms, name="norms"
    )
    return (
        grad_tokens.T,
        grad_route.T,
        grad_gate[None],
        grad_up[None],
        grad_down[None],
        gate_norms.reshape(1, width),
        up_norms.reshape(1, width),
        down_norms,
    )


def solution(mesh):
    ep, tp = ("z", "c"), ("y", "x")
    fine = Mesh(mesh.devices.reshape(12, 2, 8, 4), ep + tp)
    in_specs = (
        P(ep, tp),
        P(ep, None),
        P(ep, None),
        P(ep, tp),
        P(ep, tp, None),
        P(ep, tp, None),
        P(ep, tp, None),
    )
    out_specs = (
        P(ep, tp),
        P(ep, None),
        P(ep, tp, None),
        P(ep, tp, None),
        P(ep, tp, None),
        P(ep, None),
        P(ep, None),
        P(ep, tp),
    )
    return jax.shard_map(
        per_device, mesh=fine, in_specs=in_specs, out_specs=out_specs, check_vma=False
    )
```

```python
import jax
import jax.numpy as jnp
from jax import lax
from jax.experimental import pallas as pl
from jax.experimental.pallas import tpu as pltpu
from jax.sharding import Mesh
from jax.sharding import PartitionSpec as P


SLOTS = 16
HALF = 64
ROOM = 20 * 2**20
F32 = jnp.float32
BF16 = jnp.bfloat16


def dot(a, b, ca, cb):
    return lax.dot_general(a, b, (((ca,), (cb,)), ((), ())), preferred_element_type=F32)


def split_hi_lo(v):
    hi = v.astype(BF16)
    return hi, (v - hi.astype(F32)).astype(BF16)


def placed(routes, tokens, experts):
    ids = lax.broadcasted_iota(jnp.int32, (experts, tokens), 0)
    first = ids == routes[0:1, :]
    second = ids == routes[1:2, :]
    named = (first | second).astype(F32).astype(BF16)
    before = (
        lax.broadcasted_iota(jnp.int32, (tokens, tokens), 0)
        < lax.broadcasted_iota(jnp.int32, (tokens, tokens), 1)
    ).astype(F32).astype(BF16)
    rank = dot(named, before, 1, 0) + (ids * SLOTS).astype(F32)
    return [
        jnp.sum(jnp.where(m, rank, 0.0), axis=0, keepdims=True).astype(jnp.int32)
        for m in (first, second)
    ]


def chosen(position, slots):
    at = lax.broadcasted_iota(jnp.int32, (slots, position.shape[1]), 0)
    return (at == position).astype(F32).astype(BF16)


def dispatch_body(tokens, routes, weights, cotangent, sent, positions):
    width, count = tokens.shape
    slots = sent.shape[0]
    at = placed(routes[...], count, slots // SLOTS)
    positions[...] = jnp.concatenate(at, axis=0)
    x = tokens[...]
    g = cotangent[...].astype(F32)
    scaled = [(g * weights[k : k + 1, :]).astype(BF16) for k in range(2)]
    rows = jnp.concatenate(
        [jnp.concatenate([x, x], axis=1), jnp.concatenate(scaled, axis=1)], axis=0
    )
    pick = jnp.concatenate([chosen(p, slots) for p in at], axis=1)
    sent[...] = dot(pick, rows, 1, 1).astype(BF16)


def quarter_weights_body(here, w_gate, w_up, w_down, *outs):
    nx = len(outs)
    hid = w_gate.shape[0]

    def write(at):
        for m, w in enumerate((w_gate, w_up, w_down)):
            for d, out in enumerate(outs):
                q = (at + d) % nx
                for j in range(out.shape[1] // 128):
                    a, b = ((2 * j) * nx + q) * HALF, ((2 * j + 1) * nx + q) * HALF
                    out[m * hid : (m + 1) * hid, j * 128 : (j + 1) * 128] = jnp.concatenate(
                        [w[:, a : a + HALF], w[:, b : b + HALF]], axis=1
                    )

    for at in range(nx):
        pl.when(here[0] == at)(lambda at=at: write(at))


def partial_body(here, rows, w0, w1, w2, w3, out, x_out, s_out):
    weights = (w0, w1, w2, w3)
    nx = len(weights)
    ny = rows.shape[0]
    for j in range(ny // 2):
        a, b = rows[2 * j], rows[2 * j + 1]
        x_out[:, j * 128 : (j + 1) * 128] = jnp.concatenate([a[:, :HALF], b[:, :HALF]], axis=1)
        s_out[:, j * 128 : (j + 1) * 128] = jnp.concatenate([a[:, HALF:], b[:, HALF:]], axis=1)
    x, s = x_out[...], s_out[...]
    hid = w0.shape[0] // 3
    for d, w in enumerate(weights):
        q = (here[0] + nx - d) % nx
        out[q, : 2 * hid, :] = dot(w[: 2 * hid, :], x, 1, 1).astype(BF16)
        out[q, 2 * hid :, :] = dot(w[2 * hid :, :], s, 1, 1).astype(BF16)


def activation_body(parts, out):
    total = parts[0].astype(F32)
    for q in range(1, parts.shape[0]):
        total = total + parts[q].astype(F32)
    hid = total.shape[0] // 3
    gate, up, dhid = total[:hid], total[hid : 2 * hid], total[2 * hid :]
    sig = 1.0 / (1.0 + jnp.exp(-gate))
    active = gate * sig
    slope = sig * (1.0 + gate * (1.0 - sig))
    hidden = (active * up).astype(BF16)
    dgate = (dhid * up * slope).astype(BF16)
    dup = (dhid * active).astype(BF16)
    value = jnp.sum(hidden.astype(F32) * dhid, axis=0, keepdims=True)
    hi, lo = split_hi_lo(value)
    pad = jnp.zeros((out.shape[1] - 3 * hid - 2, out.shape[2]), BF16)
    block = jnp.concatenate([dgate, dup, hidden, hi, lo, pad], axis=0)
    for q in range(out.shape[0]):
        out[q] = block


def backward_body(here, acts, w0, w1, w2, w3, x_rows, s_rows, back, *grads):
    weights = (w0, w1, w2, w3)
    nx, ny = len(weights), back.shape[0]
    hid = w0.shape[0] // 3
    width = w0.shape[1]
    slots = acts.shape[2]
    terms = dot(w0[: 2 * hid, :], acts[here[0], : 2 * hid, :], 0, 0)
    for d in range(1, nx):
        q = (here[0] + nx - d) % nx
        terms = terms + dot(weights[d][: 2 * hid, :], acts[q, : 2 * hid, :], 0, 0)
    terms = terms.astype(BF16)
    x, s = x_rows[...], s_rows[...]
    norms = [jnp.zeros((1, width), F32) for _ in range(2)]
    value = jnp.zeros((1, slots), F32)
    for d in range(nx):
        q = (here[0] + d) % nx
        pair = dot(acts[q, : 2 * hid, :], x, 1, 0)
        down = dot(acts[q, 2 * hid : 3 * hid, :], s, 1, 0)
        grads[d][: 2 * hid, :] = pair.astype(BF16)
        grads[d][2 * hid : 3 * hid, :] = down.astype(BF16)
        for m in range(2):
            part = pair[m * hid : (m + 1) * hid]
            norms[m] = norms[m] + jnp.sum(part * part, axis=0, keepdims=True)
        tail = acts[q, 3 * hid : 3 * hid + 2, :].astype(F32)
        value = value + tail[0:1] + tail[1:2]
    lines = list(split_hi_lo(value))
    rest = jnp.zeros((1, 2 * slots - width), BF16)
    for n in norms:
        for v in split_hi_lo(n):
            lines += [v[:, :slots], jnp.concatenate([v[:, slots:], rest], axis=1)]
    pad = jnp.zeros((back.shape[1] - HALF - len(lines), slots), BF16)
    extra = jnp.concatenate(lines + [pad], axis=0)
    for j in range(ny):
        back[j, :HALF, :] = terms[j * HALF : (j + 1) * HALF]
        back[j, HALF:, :] = extra
    for out in grads:
        out[3 * hid :, :] = jnp.zeros((16, width), BF16)


def gathered_body(parts, g0, g1, g2, g3, sent, *outs):
    total = parts[0].astype(F32)
    for j in range(1, parts.shape[0]):
        total = total + parts[j].astype(F32)
    slots = total.shape[1]
    hi, lo = split_hi_lo(total[HALF : HALF + 1] + total[HALF + 1 : HALF + 2])
    pad = jnp.zeros((128 - HALF - 2, slots), F32)
    block = jnp.concatenate([total[:HALF], hi.astype(F32), lo.astype(F32), pad], axis=0)
    sent[...] = block.T.astype(BF16)
    rows, width = outs[0].shape
    lines = []
    for m in range(2):
        at = HALF + 2 + 4 * m
        one = total[at : at + 2] + total[at + 2 : at + 4]
        lines += split_hi_lo(jnp.concatenate([one[0:1], one[1:2, : width - slots]], axis=1))
    lines.append(jnp.zeros((16 - len(lines), width), BF16))
    tail = jnp.concatenate(lines, axis=0)
    for out in outs:
        out[rows - 16 :, :] = tail


def combine_body(back, positions, weights, grad_tokens, grad_route):
    slots, count = back.shape[0], positions.shape[1]
    pick = jnp.concatenate([chosen(positions[k : k + 1, :], slots) for k in range(2)], axis=1)
    got = dot(back[...], pick, 0, 0)
    grad_tokens[...] = (got[:HALF, :count] + got[:HALF, count:]).astype(BF16)
    value = got[HALF : HALF + 1] + got[HALF + 1 : HALF + 2]
    value = jnp.concatenate([value[:, :count], value[:, count:]], axis=0)
    grad_route[...] = value / weights[...]


def grads_body(
    here, p0, p1, p2, p3, grad_gate, grad_up, grad_down, gate_norms, up_norms, down_norms, parts
):
    received = (p0, p1, p2, p3)
    nx = len(received)
    for d, p in enumerate(received):
        parts[(here[0] + nx - d) % nx] = p[...]
    hid = grad_gate.shape[0]
    ny = parts.shape[2] // HALF

    def features(lines, y, h):
        at = y * HALF
        pair = [parts[2 * h + k, lines, at : at + HALF] for k in range(2)]
        return jnp.concatenate(pair, axis=1).astype(F32)

    acc = jnp.zeros((hid, 128), F32)
    for m, out in enumerate((grad_gate, grad_up, grad_down)):
        for y in range(ny):
            for h in range(nx // 2):
                tile = features(slice(m * hid, (m + 1) * hid), y, h)
                at = (y * (nx // 2) + h) * 128
                out[:, at : at + 128] = tile
                if m == 2:
                    acc = acc + tile * tile
    down_norms[...] = jnp.sum(acc.T, axis=0, keepdims=True)
    lines = [
        features(slice(3 * hid, 3 * hid + 16), y, h) for y in range(ny) for h in range(nx // 2)
    ]
    for m, out in enumerate((gate_norms, up_norms)):
        out[...] = jnp.concatenate(
            [one[2 * m : 2 * m + 1] + one[2 * m + 1 : 2 * m + 2] for one in lines], axis=0
        )


def call(body, outs, *args, name, near=(), far=False, scratch=(), aliases=None):
    smem = pl.BlockSpec(memory_space=pltpu.SMEM)
    vmem = pl.BlockSpec(memory_space=pltpu.VMEM)
    specs = [smem if a.ndim == 1 else vmem for a in args]
    args = [
        pltpu.with_memory_space_constraint(a, pltpu.VMEM) if k in near else a
        for k, a in enumerate(args)
    ]
    shape = jax.ShapeDtypeStruct if far else pltpu.VMEM
    return pl.pallas_call(
        body,
        out_shape=[shape(s, d) for s, d in outs],
        in_specs=specs,
        out_specs=[vmem] * len(outs),
        scratch_shapes=list(scratch),
        input_output_aliases=aliases or {},
        compiler_params=pltpu.CompilerParams(vmem_limit_bytes=ROOM),
        name=name,
    )(*args)


def swap(a, axis):
    return lax.all_to_all(a, axis, 0, 0, tiled=True)


def along(pieces, axis):
    n = len(pieces)
    return [pieces[0]] + [
        lax.ppermute(pieces[d], axis, [(i, (i + d) % n) for i in range(n)]) for d in range(1, n)
    ]


def per_device(tokens, routes, route_weights, grad_out, w_gate, w_up, w_down):
    ny, nx = lax.axis_size("y"), lax.axis_size("x")
    sources = lax.axis_size("z") * lax.axis_size("c")
    here = lax.axis_index("x").astype(jnp.int32).reshape(1)
    count, feat = tokens.shape
    _, hid, width = w_gate.shape
    slots = sources * SLOTS
    quarter = width // nx
    sent, positions = call(
        dispatch_body,
        [((slots, 2 * feat), BF16), ((2, count), jnp.int32)],
        tokens.T,
        routes.T,
        route_weights.T,
        grad_out.T,
        name="dispatch",
    )
    w_sent = call(
        quarter_weights_body,
        [((3 * hid, quarter), BF16)] * nx,
        here,
        w_gate[0],
        w_up[0],
        w_down[0],
        name="quarter_weights",
    )
    weights = along(w_sent, "x")
    mine = swap(sent.reshape(sources, SLOTS, 2 * feat), ("z", "c")).reshape(slots, 2 * feat)
    rows = lax.all_gather(mine, "y", axis=0, tiled=False)
    parts, x_rows, s_rows = call(
        partial_body,
        [
            ((nx, 3 * hid, slots), BF16),
            ((slots, quarter), BF16),
            ((slots, quarter), BF16),
        ],
        here,
        rows,
        *weights,
        name="partial",
        near=range(1, 6),
    )
    parts = swap(parts, "x")
    (acts,) = call(
        activation_body,
        [((nx, 3 * hid + 16, slots), BF16)],
        parts,
        name="activation",
        near=(0,),
    )
    acts = swap(acts, "x")
    back, *grads = call(
        backward_body,
        [((ny, feat + 16, slots), BF16)] + [((3 * hid + 16, quarter), BF16)] * nx,
        here,
        acts,
        *weights,
        x_rows,
        s_rows,
        name="backward",
        near=range(1, 8),
    )
    back = swap(back, "y")
    back_sent, *grads = call(
        gathered_body,
        [((slots, 128), BF16)] + [((3 * hid + 16, quarter), BF16)] * nx,
        back,
        *grads,
        name="gathered",
        near=range(0, 5),
        aliases={1: 1, 2: 2, 3: 3, 4: 4},
    )
    grads = along(grads, "x")
    back = swap(back_sent.reshape(sources, SLOTS, 128), ("z", "c")).reshape(slots, 128)
    grad_gate, grad_up, grad_down, gate_norms, up_norms, down_norms = call(
        grads_body,
        [((hid, width), F32)] * 3 + [((width // 128, 128), F32)] * 2 + [((1, hid), F32)],
        here,
        *grads,
        name="grads",
        near=range(1, 5),
        far=True,
        scratch=[pltpu.VMEM((nx, 3 * hid + 16, quarter), BF16)],
    )
    grad_tokens, grad_route = call(
        combine_body,
        [((feat, count), BF16), ((2, count), F32)],
        back,
        positions,
        route_weights.T,
        name="combine",
        near=(0, 1),
        far=True,
    )
    return (
        grad_tokens.T,
        grad_route.T,
        grad_gate[None],
        grad_up[None],
        grad_down[None],
        gate_norms.reshape(1, width),
        up_norms.reshape(1, width),
        down_norms,
    )


def solution(mesh):
    ep, tp = ("z", "c"), ("y", "x")
    fine = Mesh(mesh.devices.reshape(12, 2, 8, 4), ep + tp)
    in_specs = (
        P(ep, tp),
        P(ep, None),
        P(ep, None),
        P(ep, tp),
        P(ep, tp, None),
        P(ep, tp, None),
        P(ep, tp, None),
    )
    out_specs = (
        P(ep, tp),
        P(ep, None),
        P(ep, tp, None),
        P(ep, tp, None),
        P(ep, tp, None),
        P(ep, None),
        P(ep, None),
        P(ep, tp),
    )
    return jax.shard_map(
        per_device, mesh=fine, in_specs=in_specs, out_specs=out_specs, check_vma=False
    )
```

```python
import jax
import jax.numpy as jnp
from jax import lax
from jax.experimental import pallas as pl
from jax.experimental.pallas import tpu as pltpu
from jax.sharding import Mesh
from jax.sharding import PartitionSpec as P


SLOTS = 16
HALF = 64
ROOM = 20 * 2**20
F32 = jnp.float32
BF16 = jnp.bfloat16


def dot(a, b, ca, cb):
    return lax.dot_general(a, b, (((ca,), (cb,)), ((), ())), preferred_element_type=F32)


def split_hi_lo(v):
    hi = v.astype(BF16)
    return hi, (v - hi.astype(F32)).astype(BF16)


def placed(routes, tokens, experts):
    ids = lax.broadcasted_iota(jnp.int32, (experts, tokens), 0)
    first = ids == routes[0:1, :]
    second = ids == routes[1:2, :]
    named = (first | second).astype(F32).astype(BF16)
    before = (
        lax.broadcasted_iota(jnp.int32, (tokens, tokens), 0)
        < lax.broadcasted_iota(jnp.int32, (tokens, tokens), 1)
    ).astype(F32).astype(BF16)
    rank = dot(named, before, 1, 0) + (ids * SLOTS).astype(F32)
    return [
        jnp.sum(jnp.where(m, rank, 0.0), axis=0, keepdims=True).astype(jnp.int32)
        for m in (first, second)
    ]


def chosen(position, slots):
    at = lax.broadcasted_iota(jnp.int32, (slots, position.shape[1]), 0)
    return (at == position).astype(F32).astype(BF16)


def fetched(sources, targets, sems):
    copies = [
        pltpu.make_async_copy(a, b, sems.at[k]) for k, (a, b) in enumerate(zip(sources, targets))
    ]
    for c in copies:
        c.start()
    return copies


def dispatch_body(
    tokens_far,
    routes_far,
    weights_far,
    cotangent_far,
    sent,
    positions,
    weights,
    tokens,
    routes,
    cotangent,
    sems,
):
    far = (tokens_far, routes_far, weights_far, cotangent_far)
    for c in fetched(far, (tokens, routes, weights, cotangent), sems):
        c.wait()
    width, count = tokens.shape
    slots = sent.shape[0]
    at = placed(routes[...], count, slots // SLOTS)
    positions[...] = jnp.concatenate(at, axis=0)
    x = tokens[...]
    g = cotangent[...].astype(F32)
    scaled = [(g * weights[k : k + 1, :]).astype(BF16) for k in range(2)]
    rows = jnp.concatenate(
        [jnp.concatenate([x, x], axis=1), jnp.concatenate(scaled, axis=1)], axis=0
    )
    pick = jnp.concatenate([chosen(p, slots) for p in at], axis=1)
    sent[...] = dot(pick, rows, 1, 1).astype(BF16)


def quarter_weights_body(here, f_gate, f_up, f_down, o0, o1, o2, o3, w_gate, w_up, w_down, sems):
    for c in fetched((f_gate, f_up, f_down), (w_gate, w_up, w_down), sems):
        c.wait()
    outs = (o0, o1, o2, o3)
    nx = len(outs)
    hid = w_gate.shape[0]

    def write(at):
        for m, w in enumerate((w_gate, w_up, w_down)):
            for d, out in enumerate(outs):
                q = (at + d) % nx
                for j in range(out.shape[1] // 128):
                    a, b = ((2 * j) * nx + q) * HALF, ((2 * j + 1) * nx + q) * HALF
                    out[m * hid : (m + 1) * hid, j * 128 : (j + 1) * 128] = jnp.concatenate(
                        [w[:, a : a + HALF], w[:, b : b + HALF]], axis=1
                    )

    for at in range(nx):
        pl.when(here[0] == at)(lambda at=at: write(at))


def partial_body(here, rows, w0, w1, w2, w3, out, x_out, s_out):
    weights = (w0, w1, w2, w3)
    nx = len(weights)
    ny = rows.shape[0]
    for j in range(ny // 2):
        a, b = rows[2 * j], rows[2 * j + 1]
        x_out[:, j * 128 : (j + 1) * 128] = jnp.concatenate([a[:, :HALF], b[:, :HALF]], axis=1)
        s_out[:, j * 128 : (j + 1) * 128] = jnp.concatenate([a[:, HALF:], b[:, HALF:]], axis=1)
    x, s = x_out[...], s_out[...]
    hid = w0.shape[0] // 3
    for d, w in enumerate(weights):
        q = (here[0] + nx - d) % nx
        out[q, : 2 * hid, :] = dot(w[: 2 * hid, :], x, 1, 1).astype(BF16)
        out[q, 2 * hid :, :] = dot(w[2 * hid :, :], s, 1, 1).astype(BF16)


def activation_body(parts, out):
    total = parts[0].astype(F32)
    for q in range(1, parts.shape[0]):
        total = total + parts[q].astype(F32)
    hid = total.shape[0] // 3
    gate, up, dhid = total[:hid], total[hid : 2 * hid], total[2 * hid :]
    sig = 1.0 / (1.0 + jnp.exp(-gate))
    active = gate * sig
    slope = sig * (1.0 + gate * (1.0 - sig))
    hidden = (active * up).astype(BF16)
    dgate = (dhid * up * slope).astype(BF16)
    dup = (dhid * active).astype(BF16)
    value = jnp.sum(hidden.astype(F32) * dhid, axis=0, keepdims=True)
    hi, lo = split_hi_lo(value)
    pad = jnp.zeros((out.shape[1] - 3 * hid - 2, out.shape[2]), BF16)
    block = jnp.concatenate([dgate, dup, hidden, hi, lo, pad], axis=0)
    for q in range(out.shape[0]):
        out[q] = block


def backward_body(here, acts, w0, w1, w2, w3, x_rows, s_rows, back, *grads):
    weights = (w0, w1, w2, w3)
    nx, ny = len(weights), back.shape[0]
    hid = w0.shape[0] // 3
    width = w0.shape[1]
    slots = acts.shape[2]
    terms = dot(w0[: 2 * hid, :], acts[here[0], : 2 * hid, :], 0, 0)
    for d in range(1, nx):
        q = (here[0] + nx - d) % nx
        terms = terms + dot(weights[d][: 2 * hid, :], acts[q, : 2 * hid, :], 0, 0)
    terms = terms.astype(BF16)
    x, s = x_rows[...], s_rows[...]
    norms = [jnp.zeros((1, width), F32) for _ in range(2)]
    value = jnp.zeros((1, slots), F32)
    for d in range(nx):
        q = (here[0] + d) % nx
        pair = dot(acts[q, : 2 * hid, :], x, 1, 0)
        down = dot(acts[q, 2 * hid : 3 * hid, :], s, 1, 0)
        grads[d][: 2 * hid, :] = pair.astype(BF16)
        grads[d][2 * hid :, :] = down.astype(BF16)
        for m in range(2):
            part = pair[m * hid : (m + 1) * hid]
            norms[m] = norms[m] + jnp.sum(part * part, axis=0, keepdims=True)
        tail = acts[q, 3 * hid : 3 * hid + 2, :].astype(F32)
        value = value + tail[0:1] + tail[1:2]
    flat = [v for n in norms for v in split_hi_lo(n)]
    lines = list(split_hi_lo(value))
    spare = (back.shape[1] - HALF - len(lines)) * slots - len(flat) * width
    flat = jnp.concatenate(flat + [jnp.zeros((1, spare), BF16)], axis=1)
    lines += [flat[:, k : k + slots] for k in range(0, flat.shape[1], slots)]
    extra = jnp.concatenate(lines, axis=0)
    for j in range(ny):
        back[j, :HALF, :] = terms[j * HALF : (j + 1) * HALF]
        back[j, HALF:, :] = extra


def gathered_body(parts, sent, norms):
    total = parts[0].astype(F32)
    for j in range(1, parts.shape[0]):
        total = total + parts[j].astype(F32)
    slots = total.shape[1]
    hi, lo = split_hi_lo(total[HALF : HALF + 1] + total[HALF + 1 : HALF + 2])
    pad = jnp.zeros((128 - HALF - 2, slots), F32)
    block = jnp.concatenate([total[:HALF], hi.astype(F32), lo.astype(F32), pad], axis=0)
    sent[...] = block.T.astype(BF16)
    flat = jnp.concatenate([total[k : k + 1] for k in range(HALF + 2, total.shape[0])], axis=1)
    tiles = [flat[:, k : k + 128] for k in range(0, flat.shape[1], 128)]
    each = norms.shape[0] // 2
    norms[...] = jnp.concatenate(
        [tiles[2 * m * each + k] + tiles[(2 * m + 1) * each + k] for m in range(2) for k in range(each)],
        axis=0,
    )


def halves(parts, lines, y, h):
    at = (y * HALF) % parts.shape[2]
    pair = [parts[2 * h + k, lines, at : at + HALF] for k in range(2)]
    return jnp.concatenate(pair, axis=1).astype(F32)


def grads_body(here, p0, p1, p2, p3, grad_gate, grad_up, grad_down, down_norms, parts):
    received = (p0, p1, p2, p3)
    nx = len(received)
    for d, p in enumerate(received):
        parts[(here[0] + nx - d) % nx] = p[...]
    hid = grad_gate.shape[0]
    acc = jnp.zeros((hid, 128), F32)
    for m, out in enumerate((grad_gate, grad_up, grad_down)):
        for y in range(parts.shape[2] // HALF):
            for h in range(nx // 2):
                tile = halves(parts, slice(m * hid, (m + 1) * hid), y, h)
                at = (y * (nx // 2) + h) * 128
                out[:, at : at + 128] = tile
                if m == 2:
                    acc = acc + tile * tile
    down_norms[...] = jnp.sum(acc.T, axis=0, keepdims=True)


def combine_body(
    here,
    back,
    positions,
    weights,
    n0,
    n1,
    n2,
    n3,
    grad_tokens,
    grad_route,
    gate_norms,
    up_norms,
    parts,
):
    slots, count = back.shape[0], positions.shape[1]
    pick = jnp.concatenate([chosen(positions[k : k + 1, :], slots) for k in range(2)], axis=1)
    got = dot(back[...], pick, 0, 0)
    grad_tokens[...] = (got[:HALF, :count] + got[:HALF, count:]).astype(BF16)
    value = got[HALF : HALF + 1] + got[HALF + 1 : HALF + 2]
    value = jnp.concatenate([value[:, :count], value[:, count:]], axis=0)
    grad_route[...] = value / weights[...]
    received = (n0, n1, n2, n3)
    nx = len(received)
    for d, n in enumerate(received):
        parts[(here[0] + nx - d) % nx] = n[...]
    each = n0.shape[0] // 2
    for m, out in enumerate((gate_norms, up_norms)):
        out[...] = jnp.concatenate(
            [
                halves(parts, slice(m * each + y // 2, m * each + y // 2 + 1), y, h)
                for y in range(2 * each)
                for h in range(nx // 2)
            ],
            axis=0,
        )


def call(body, outs, *args, name, fetch=False, far=False, scratch=()):
    smem = pl.BlockSpec(memory_space=pltpu.SMEM)
    vmem = pl.BlockSpec(memory_space=pltpu.VMEM)
    space = pltpu.HBM if fetch else pltpu.VMEM
    specs = [smem if a.ndim == 1 else pl.BlockSpec(memory_space=space) for a in args]
    args = [a if a.ndim == 1 else pltpu.with_memory_space_constraint(a, space) for a in args]
    shape = jax.ShapeDtypeStruct if far else pltpu.VMEM
    return pl.pallas_call(
        body,
        out_shape=[shape(s, d) for s, d in outs],
        in_specs=specs,
        out_specs=[vmem] * len(outs),
        scratch_shapes=list(scratch),
        compiler_params=pltpu.CompilerParams(vmem_limit_bytes=ROOM),
        name=name,
    )(*args)


def swap(a, axis):
    return lax.all_to_all(a, axis, 0, 0, tiled=True)


def along(pieces, axis):
    n = len(pieces)
    return [pieces[0]] + [
        lax.ppermute(pieces[d], axis, [(i, (i + d) % n) for i in range(n)]) for d in range(1, n)
    ]


def per_device(tokens, routes, route_weights, grad_out, w_gate, w_up, w_down):
    ny, nx = lax.axis_size("y"), lax.axis_size("x")
    sources = lax.axis_size("z") * lax.axis_size("c")
    here = lax.axis_index("x").astype(jnp.int32).reshape(1)
    count, feat = tokens.shape
    _, hid, width = w_gate.shape
    slots = sources * SLOTS
    quarter = width // nx
    small = [tokens.T, routes.T, route_weights.T, grad_out.T]
    sent, positions, scales = call(
        dispatch_body,
        [((slots, 2 * feat), BF16), ((2, count), jnp.int32), ((2, count), F32)],
        *small,
        name="dispatch",
        fetch=True,
        scratch=[pltpu.VMEM(small[k].shape, small[k].dtype) for k in (0, 1, 3)]
        + [pltpu.SemaphoreType.DMA((4,))],
    )
    w_sent = call(
        quarter_weights_body,
        [((3 * hid, quarter), BF16)] * nx,
        here,
        w_gate[0],
        w_up[0],
        w_down[0],
        name="quarter_weights",
        fetch=True,
        scratch=[pltpu.VMEM((hid, width), BF16)] * 3 + [pltpu.SemaphoreType.DMA((3,))],
    )
    mine = swap(sent.reshape(sources, SLOTS, 2 * feat), ("z", "c")).reshape(slots, 2 * feat)
    mine, w_sent = lax.optimization_barrier((mine, w_sent))
    weights = along(w_sent, "x")
    rows = swap(jnp.broadcast_to(mine[None], (ny, slots, 2 * feat)), "y")
    parts, x_rows, s_rows = call(
        partial_body,
        [
            ((nx, 3 * hid, slots), BF16),
            ((slots, quarter), BF16),
            ((slots, quarter), BF16),
        ],
        here,
        rows,
        *weights,
        name="partial",
    )
    parts = swap(parts, "x")
    (acts,) = call(
        activation_body, [((nx, 3 * hid + 16, slots), BF16)], parts, name="activation"
    )
    acts = swap(acts, "x")
    back, *grads = call(
        backward_body,
        [((ny, feat + 8, slots), BF16)] + [((3 * hid, quarter), BF16)] * nx,
        here,
        acts,
        *weights,
        x_rows,
        s_rows,
        name="backward",
    )
    grads = along(grads, "x")
    back = swap(back, "y")
    back, grads = lax.optimization_barrier((back, grads))
    back_sent, norms = call(
        gathered_body,
        [((slots, 128), BF16), ((quarter // 64, 128), F32)],
        back,
        name="gathered",
    )
    norms = along([norms] * nx, "x")
    back = swap(back_sent.reshape(sources, SLOTS, 128), ("z", "c")).reshape(slots, 128)
    grad_gate, grad_up, grad_down, down_norms = call(
        grads_body,
        [((hid, width), F32)] * 3 + [((1, hid), F32)],
        here,
        *grads,
        name="grads",
        far=True,
        scratch=[pltpu.VMEM((nx, 3 * hid, quarter), BF16)],
    )
    grad_tokens, grad_route, gate_norms, up_norms = call(
        combine_body,
        [((feat, count), BF16), ((2, count), F32)] + [((width // 128, 128), F32)] * 2,
        here,
        back,
        positions,
        scales,
        *norms,
        name="combine",
        far=True,
        scratch=[pltpu.VMEM((nx, quarter // 64, 128), F32)],
    )
    return (
        grad_tokens.T,
        grad_route.T,
        grad_gate[None],
        grad_up[None],
        grad_down[None],
        gate_norms.reshape(1, width),
        up_norms.reshape(1, width),
        down_norms,
    )


def solution(mesh):
    ep, tp = ("z", "c"), ("y", "x")
    fine = Mesh(mesh.devices.reshape(12, 2, 8, 4), ep + tp)
    in_specs = (
        P(ep, tp),
        P(ep, None),
        P(ep, None),
        P(ep, tp),
        P(ep, tp, None),
        P(ep, tp, None),
        P(ep, tp, None),
    )
    out_specs = (
        P(ep, tp),
        P(ep, None),
        P(ep, tp, None),
        P(ep, tp, None),
        P(ep, tp, None),
        P(ep, None),
        P(ep, None),
        P(ep, tp),
    )
    return jax.shard_map(
        per_device, mesh=fine, in_specs=in_specs, out_specs=out_specs, check_vma=False
    )
```

```python
import jax
import jax.numpy as jnp
from jax import lax
from jax.experimental import pallas as pl
from jax.experimental.pallas import tpu as pltpu
from jax.sharding import Mesh
from jax.sharding import PartitionSpec as P


SLOTS = 16
HALF = 64
ROOM = 20 * 2**20
F32 = jnp.float32
BF16 = jnp.bfloat16


def dot(a, b, ca, cb):
    return lax.dot_general(a, b, (((ca,), (cb,)), ((), ())), preferred_element_type=F32)


def split_hi_lo(v):
    hi = v.astype(BF16)
    return hi, (v - hi.astype(F32)).astype(BF16)


def placed(routes, tokens, experts):
    ids = lax.broadcasted_iota(jnp.int32, (experts, tokens), 0)
    first = ids == routes[0:1, :]
    second = ids == routes[1:2, :]
    named = (first | second).astype(F32).astype(BF16)
    before = (
        lax.broadcasted_iota(jnp.int32, (tokens, tokens), 0)
        < lax.broadcasted_iota(jnp.int32, (tokens, tokens), 1)
    ).astype(F32).astype(BF16)
    rank = dot(named, before, 1, 0) + (ids * SLOTS).astype(F32)
    return [
        jnp.sum(jnp.where(m, rank, 0.0), axis=0, keepdims=True).astype(jnp.int32)
        for m in (first, second)
    ]


def chosen(position, slots):
    at = lax.broadcasted_iota(jnp.int32, (slots, position.shape[1]), 0)
    return (at == position).astype(F32).astype(BF16)


def fetched(sources, targets, sems):
    copies = [
        pltpu.make_async_copy(a, b, sems.at[k]) for k, (a, b) in enumerate(zip(sources, targets))
    ]
    for c in copies:
        c.start()
    return copies


def dispatch_body(
    tokens_far,
    routes_far,
    weights_far,
    cotangent_far,
    sent,
    positions,
    weights,
    tokens,
    routes,
    cotangent,
    sems,
):
    far = (tokens_far, routes_far, weights_far, cotangent_far)
    for c in fetched(far, (tokens, routes, weights, cotangent), sems):
        c.wait()
    width, count = tokens.shape
    slots = sent.shape[0]
    at = placed(routes[...], count, slots // SLOTS)
    positions[...] = jnp.concatenate(at, axis=0)
    x = tokens[...]
    g = cotangent[...].astype(F32)
    scaled = [(g * weights[k : k + 1, :]).astype(BF16) for k in range(2)]
    rows = jnp.concatenate(
        [jnp.concatenate([x, x], axis=1), jnp.concatenate(scaled, axis=1)], axis=0
    )
    pick = jnp.concatenate([chosen(p, slots) for p in at], axis=1)
    sent[...] = dot(pick, rows, 1, 1).astype(BF16)


def quarter_weights_body(here, f_gate, f_up, f_down, o0, o1, o2, o3, w_gate, w_up, w_down, sems):
    for c in fetched((f_gate, f_up, f_down), (w_gate, w_up, w_down), sems):
        c.wait()
    outs = (o0, o1, o2, o3)
    nx = len(outs)
    hid = w_gate.shape[0]

    def write(at):
        for m, w in enumerate((w_gate, w_up, w_down)):
            for d, out in enumerate(outs):
                q = (at + d) % nx
                for j in range(out.shape[1] // 128):
                    a, b = ((2 * j) * nx + q) * HALF, ((2 * j + 1) * nx + q) * HALF
                    out[m * hid : (m + 1) * hid, j * 128 : (j + 1) * 128] = jnp.concatenate(
                        [w[:, a : a + HALF], w[:, b : b + HALF]], axis=1
                    )

    for at in range(nx):
        pl.when(here[0] == at)(lambda at=at: write(at))


def partial_body(here, rows, w0, w1, w2, w3, out, x_out, s_out):
    weights = (w0, w1, w2, w3)
    nx = len(weights)
    ny = rows.shape[0]
    for j in range(ny // 2):
        a, b = rows[2 * j], rows[2 * j + 1]
        x_out[:, j * 128 : (j + 1) * 128] = jnp.concatenate([a[:, :HALF], b[:, :HALF]], axis=1)
        s_out[:, j * 128 : (j + 1) * 128] = jnp.concatenate([a[:, HALF:], b[:, HALF:]], axis=1)
    x, s = x_out[...], s_out[...]
    hid = w0.shape[0] // 3
    for d, w in enumerate(weights):
        q = (here[0] + nx - d) % nx
        out[q, : 2 * hid, :] = dot(w[: 2 * hid, :], x, 1, 1).astype(BF16)
        out[q, 2 * hid :, :] = dot(w[2 * hid :, :], s, 1, 1).astype(BF16)


def activation_body(parts, out):
    total = parts[0].astype(F32)
    for q in range(1, parts.shape[0]):
        total = total + parts[q].astype(F32)
    hid = total.shape[0] // 3
    gate, up, dhid = total[:hid], total[hid : 2 * hid], total[2 * hid :]
    sig = 1.0 / (1.0 + jnp.exp(-gate))
    active = gate * sig
    slope = sig * (1.0 + gate * (1.0 - sig))
    hidden = (active * up).astype(BF16)
    dgate = (dhid * up * slope).astype(BF16)
    dup = (dhid * active).astype(BF16)
    value = jnp.sum(hidden.astype(F32) * dhid, axis=0, keepdims=True)
    hi, lo = split_hi_lo(value)
    pad = jnp.zeros((out.shape[1] - 3 * hid - 2, out.shape[2]), BF16)
    block = jnp.concatenate([dgate, dup, hidden, hi, lo, pad], axis=0)
    for q in range(out.shape[0]):
        out[q] = block


def backward_body(here, acts, w0, w1, w2, w3, x_rows, s_rows, back, *grads):
    weights = (w0, w1, w2, w3)
    nx, ny = len(weights), back.shape[0]
    hid = w0.shape[0] // 3
    width = w0.shape[1]
    slots = acts.shape[2]
    terms = dot(w0[: 2 * hid, :], acts[here[0], : 2 * hid, :], 0, 0)
    for d in range(1, nx):
        q = (here[0] + nx - d) % nx
        terms = terms + dot(weights[d][: 2 * hid, :], acts[q, : 2 * hid, :], 0, 0)
    terms = terms.astype(BF16)
    x, s = x_rows[...], s_rows[...]
    norms = [jnp.zeros((1, width), F32) for _ in range(2)]
    value = jnp.zeros((1, slots), F32)
    for d in range(nx):
        q = (here[0] + d) % nx
        pair = dot(acts[q, : 2 * hid, :], x, 1, 0)
        down = dot(acts[q, 2 * hid : 3 * hid, :], s, 1, 0)
        grads[d][: 2 * hid, :] = pair.astype(BF16)
        grads[d][2 * hid : 3 * hid, :] = down.astype(BF16)
        for m in range(2):
            part = pair[m * hid : (m + 1) * hid]
            norms[m] = norms[m] + jnp.sum(part * part, axis=0, keepdims=True)
        tail = acts[q, 3 * hid : 3 * hid + 2, :].astype(F32)
        value = value + tail[0:1] + tail[1:2]
    flat = [v for n in norms for v in split_hi_lo(n)]
    lines = list(split_hi_lo(value))
    spare = (back.shape[1] - HALF - len(lines)) * slots - len(flat) * width
    flat = jnp.concatenate(flat + [jnp.zeros((1, spare), BF16)], axis=1)
    lines += [flat[:, k : k + slots] for k in range(0, flat.shape[1], slots)]
    extra = jnp.concatenate(lines, axis=0)
    for j in range(ny):
        back[j, :HALF, :] = terms[j * HALF : (j + 1) * HALF]
        back[j, HALF:, :] = extra


def gathered_body(parts, far, sent, norms, far_out):
    total = parts[0].astype(F32)
    for j in range(1, parts.shape[0]):
        total = total + parts[j].astype(F32)
    slots = total.shape[1]
    hi, lo = split_hi_lo(total[HALF : HALF + 1] + total[HALF + 1 : HALF + 2])
    pad = jnp.zeros((128 - HALF - 2, slots), F32)
    block = jnp.concatenate([total[:HALF], hi.astype(F32), lo.astype(F32), pad], axis=0)
    sent[...] = block.T.astype(BF16)
    flat = jnp.concatenate([total[k : k + 1] for k in range(HALF + 2, total.shape[0])], axis=1)
    tiles = [flat[:, k : k + 128] for k in range(0, flat.shape[1], 128)]
    each = norms.shape[0] // 2
    lines = [
        tiles[2 * m * each + k] + tiles[(2 * m + 1) * each + k]
        for m in range(2)
        for k in range(each)
    ]
    norms[...] = jnp.concatenate(lines, axis=0)
    both = [jnp.concatenate(lines[m * each : (m + 1) * each], axis=1) for m in range(2)]
    rows, width = far_out.shape
    tail = [v for n in both for v in split_hi_lo(n)] + [jnp.zeros((12, width), BF16)]
    far_out[rows - 16 :, :] = jnp.concatenate(tail, axis=0)


def halves(parts, lines, y, h):
    at = (y * HALF) % parts.shape[2]
    pair = [parts[2 * h + k, lines, at : at + HALF] for k in range(2)]
    return jnp.concatenate(pair, axis=1).astype(F32)


def grads_body(here, p0, p1, p2, p3, grad_gate, grad_up, grad_down, down_norms, parts):
    received = (p0, p1, p2, p3)
    nx = len(received)
    hid = grad_gate.shape[0]
    for d, p in enumerate(received):
        parts[(here[0] + nx - d) % nx] = p[: 3 * hid, :]
    acc = jnp.zeros((hid, 128), F32)
    for m, out in enumerate((grad_gate, grad_up, grad_down)):
        for y in range(parts.shape[2] // HALF):
            for h in range(nx // 2):
                tile = halves(parts, slice(m * hid, (m + 1) * hid), y, h)
                at = (y * (nx // 2) + h) * 128
                out[:, at : at + 128] = tile
                if m == 2:
                    acc = acc + tile * tile
    down_norms[...] = jnp.sum(acc.T, axis=0, keepdims=True)


def combine_body(
    here,
    back,
    positions,
    weights,
    n0,
    n1,
    far,
    n3,
    grad_tokens,
    grad_route,
    gate_norms,
    up_norms,
    parts,
):
    slots, count = back.shape[0], positions.shape[1]
    pick = jnp.concatenate([chosen(positions[k : k + 1, :], slots) for k in range(2)], axis=1)
    got = dot(back[...], pick, 0, 0)
    grad_tokens[...] = (got[:HALF, :count] + got[:HALF, count:]).astype(BF16)
    value = got[HALF : HALF + 1] + got[HALF + 1 : HALF + 2]
    value = jnp.concatenate([value[:, :count], value[:, count:]], axis=0)
    grad_route[...] = value / weights[...]
    nx = parts.shape[0]
    for d, n in ((0, n0), (1, n1), (3, n3)):
        parts[(here[0] + nx - d) % nx] = n[...]
    each = n0.shape[0] // 2
    tail = far[far.shape[0] - 16 :, :].astype(F32)
    both = [tail[2 * m : 2 * m + 1] + tail[2 * m + 1 : 2 * m + 2] for m in range(2)]
    parts[(here[0] + nx - 2) % nx] = jnp.concatenate(
        [v[:, k * 128 : (k + 1) * 128] for v in both for k in range(each)], axis=0
    )
    for m, out in enumerate((gate_norms, up_norms)):
        out[...] = jnp.concatenate(
            [
                halves(parts, slice(m * each + y // 2, m * each + y // 2 + 1), y, h)
                for y in range(2 * each)
                for h in range(nx // 2)
            ],
            axis=0,
        )


def call(body, outs, *args, name, fetch=False, far=False, scratch=(), aliases=None):
    smem = pl.BlockSpec(memory_space=pltpu.SMEM)
    vmem = pl.BlockSpec(memory_space=pltpu.VMEM)
    space = pltpu.HBM if fetch else pltpu.VMEM
    specs = [smem if a.ndim == 1 else pl.BlockSpec(memory_space=space) for a in args]
    args = [a if a.ndim == 1 else pltpu.with_memory_space_constraint(a, space) for a in args]
    shape = jax.ShapeDtypeStruct if far else pltpu.VMEM
    return pl.pallas_call(
        body,
        out_shape=[shape(s, d) for s, d in outs],
        in_specs=specs,
        out_specs=[vmem] * len(outs),
        scratch_shapes=list(scratch),
        input_output_aliases=aliases or {},
        compiler_params=pltpu.CompilerParams(vmem_limit_bytes=ROOM),
        name=name,
    )(*args)


def swap(a, axis):
    return lax.all_to_all(a, axis, 0, 0, tiled=True)


def shifted(piece, axis, d):
    n = lax.axis_size(axis)
    return lax.ppermute(piece, axis, [(i, (i + d) % n) for i in range(n)])


def per_device(tokens, routes, route_weights, grad_out, w_gate, w_up, w_down):
    ny, nx = lax.axis_size("y"), lax.axis_size("x")
    sources = lax.axis_size("z") * lax.axis_size("c")
    here = lax.axis_index("x").astype(jnp.int32).reshape(1)
    count, feat = tokens.shape
    _, hid, width = w_gate.shape
    slots = sources * SLOTS
    quarter = width // nx
    small = [tokens.T, routes.T, route_weights.T, grad_out.T]
    sent, positions, scales = call(
        dispatch_body,
        [((slots, 2 * feat), BF16), ((2, count), jnp.int32), ((2, count), F32)],
        *small,
        name="dispatch",
        fetch=True,
        scratch=[pltpu.VMEM(small[k].shape, small[k].dtype) for k in (0, 1, 3)]
        + [pltpu.SemaphoreType.DMA((4,))],
    )
    w_sent = call(
        quarter_weights_body,
        [((3 * hid, quarter), BF16)] * nx,
        here,
        w_gate[0],
        w_up[0],
        w_down[0],
        name="quarter_weights",
        fetch=True,
        scratch=[pltpu.VMEM((hid, width), BF16)] * 3 + [pltpu.SemaphoreType.DMA((3,))],
    )
    mine = swap(sent.reshape(sources, SLOTS, 2 * feat), ("z", "c")).reshape(slots, 2 * feat)
    weights = [w_sent[0]] + [shifted(w_sent[d], "x", d) for d in range(1, nx)]
    rows = lax.all_gather(mine, "y", axis=0, tiled=False)
    parts, x_rows, s_rows = call(
        partial_body,
        [
            ((nx, 3 * hid, slots), BF16),
            ((slots, quarter), BF16),
            ((slots, quarter), BF16),
        ],
        here,
        rows,
        *weights,
        name="partial",
    )
    parts = swap(parts, "x")
    (acts,) = call(
        activation_body, [((nx, 3 * hid + 8, slots), BF16)], parts, name="activation"
    )
    acts = swap(acts, "x")
    back, *grads = call(
        backward_body,
        [((ny, feat + 8, slots), BF16)]
        + [((3 * hid + (16 if d == 2 else 0), quarter), BF16) for d in range(nx)],
        here,
        acts,
        *weights,
        x_rows,
        s_rows,
        name="backward",
    )
    near = [shifted(grads[d], "x", d) for d in (1, 3)]
    back = swap(back, "y")
    back, near = lax.optimization_barrier((back, near))
    back_sent, norms, far = call(
        gathered_body,
        [
            ((slots, 128), BF16),
            ((quarter // 64, 128), F32),
            ((3 * hid + 16, quarter), BF16),
        ],
        back,
        grads[2],
        name="gathered",
        aliases={1: 2},
    )
    far = shifted(far, "x", 2)
    norms = [norms, shifted(norms, "x", 1), far, shifted(norms, "x", 3)]
    grads = [grads[0], near[0], far, near[1]]
    back = swap(back_sent.reshape(sources, SLOTS, 128), ("z", "c")).reshape(slots, 128)
    grad_gate, grad_up, grad_down, down_norms = call(
        grads_body,
        [((hid, width), F32)] * 3 + [((1, hid), F32)],
        here,
        *grads,
        name="grads",
        far=True,
        scratch=[pltpu.VMEM((nx, 3 * hid, quarter), BF16)],
    )
    grad_tokens, grad_route, gate_norms, up_norms = call(
        combine_body,
        [((feat, count), BF16), ((2, count), F32)] + [((width // 128, 128), F32)] * 2,
        here,
        back,
        positions,
        scales,
        *norms,
        name="combine",
        far=True,
        scratch=[pltpu.VMEM((nx, quarter // 64, 128), F32)],
    )
    return (
        grad_tokens.T,
        grad_route.T,
        grad_gate[None],
        grad_up[None],
        grad_down[None],
        gate_norms.reshape(1, width),
        up_norms.reshape(1, width),
        down_norms,
    )


def solution(mesh):
    ep, tp = ("z", "c"), ("y", "x")
    fine = Mesh(mesh.devices.reshape(12, 2, 8, 4), ep + tp)
    in_specs = (
        P(ep, tp),
        P(ep, None),
        P(ep, None),
        P(ep, tp),
        P(ep, tp, None),
        P(ep, tp, None),
        P(ep, tp, None),
    )
    out_specs = (
        P(ep, tp),
        P(ep, None),
        P(ep, tp, None),
        P(ep, tp, None),
        P(ep, tp, None),
        P(ep, None),
        P(ep, None),
        P(ep, tp),
    )
    return jax.shard_map(
        per_device, mesh=fine, in_specs=in_specs, out_specs=out_specs, check_vma=False
    )
```

```python
import jax
import jax.numpy as jnp
from jax import lax
from jax.experimental import pallas as pl
from jax.experimental.pallas import tpu as pltpu
from jax.sharding import Mesh
from jax.sharding import PartitionSpec as P


SLOTS = 16
HALF = 64
ROOM = 20 * 2**20
F32 = jnp.float32
BF16 = jnp.bfloat16


def dot(a, b, ca, cb):
    return lax.dot_general(a, b, (((ca,), (cb,)), ((), ())), preferred_element_type=F32)


def split_hi_lo(v):
    hi = v.astype(BF16)
    return hi, (v - hi.astype(F32)).astype(BF16)


def placed(routes, tokens, experts):
    ids = lax.broadcasted_iota(jnp.int32, (experts, tokens), 0)
    first = ids == routes[0:1, :]
    second = ids == routes[1:2, :]
    named = (first | second).astype(F32).astype(BF16)
    before = (
        lax.broadcasted_iota(jnp.int32, (tokens, tokens), 0)
        < lax.broadcasted_iota(jnp.int32, (tokens, tokens), 1)
    ).astype(F32).astype(BF16)
    rank = dot(named, before, 1, 0) + (ids * SLOTS).astype(F32)
    return [
        jnp.sum(jnp.where(m, rank, 0.0), axis=0, keepdims=True).astype(jnp.int32)
        for m in (first, second)
    ]


def chosen(position, slots):
    at = lax.broadcasted_iota(jnp.int32, (slots, position.shape[1]), 0)
    return (at == position).astype(F32).astype(BF16)


def fetched(sources, targets, sems):
    copies = [
        pltpu.make_async_copy(a, b, sems.at[k]) for k, (a, b) in enumerate(zip(sources, targets))
    ]
    for c in copies:
        c.start()
    return copies


def dispatch_body(
    tokens_far,
    routes_far,
    weights_far,
    cotangent_far,
    sent,
    positions,
    weights,
    tokens,
    routes,
    cotangent,
    sems,
):
    far = (tokens_far, routes_far, weights_far, cotangent_far)
    for c in fetched(far, (tokens, routes, weights, cotangent), sems):
        c.wait()
    _, count = tokens.shape
    slots = sent.shape[0]
    at = placed(routes[...], count, slots // SLOTS)
    positions[...] = jnp.concatenate(at, axis=0)
    x = tokens[...]
    g = cotangent[...].astype(F32)
    scaled = [(g * weights[k : k + 1, :]).astype(BF16) for k in range(2)]
    rows = jnp.concatenate(
        [jnp.concatenate([x, x], axis=1), jnp.concatenate(scaled, axis=1)], axis=0
    )
    pick = jnp.concatenate([chosen(p, slots) for p in at], axis=1)
    sent[...] = dot(pick, rows, 1, 1).astype(BF16)


def quarter_weights_body(here, f_gate, f_up, f_down, o0, o1, o2, o3, w_gate, w_up, w_down, sems):
    for c in fetched((f_gate, f_up, f_down), (w_gate, w_up, w_down), sems):
        c.wait()
    outs = (o0, o1, o2, o3)
    nx = len(outs)
    hid = w_gate.shape[0]

    def write(at):
        for m, w in enumerate((w_gate, w_up, w_down)):
            for d, out in enumerate(outs):
                q = (at + d) % nx
                for j in range(out.shape[1] // 128):
                    a, b = ((2 * j) * nx + q) * HALF, ((2 * j + 1) * nx + q) * HALF
                    out[m * hid : (m + 1) * hid, j * 128 : (j + 1) * 128] = jnp.concatenate(
                        [w[:, a : a + HALF], w[:, b : b + HALF]], axis=1
                    )

    for at in range(nx):
        pl.when(here[0] == at)(lambda at=at: write(at))


def copies_body(one, out):
    for k in range(out.shape[0]):
        out[k] = one[...]


def partial_body(here, rows, w0, w1, w2, w3, out, x_out, s_out):
    weights = (w0, w1, w2, w3)
    nx = len(weights)
    ny = rows.shape[0]
    for j in range(ny // 2):
        a, b = rows[2 * j], rows[2 * j + 1]
        x_out[:, j * 128 : (j + 1) * 128] = jnp.concatenate([a[:, :HALF], b[:, :HALF]], axis=1)
        s_out[:, j * 128 : (j + 1) * 128] = jnp.concatenate([a[:, HALF:], b[:, HALF:]], axis=1)
    x, s = x_out[...], s_out[...]
    hid = w0.shape[0] // 3
    for d, w in enumerate(weights):
        q = (here[0] + nx - d) % nx
        out[q, : 2 * hid, :] = dot(w[: 2 * hid, :], x, 1, 1).astype(BF16)
        out[q, 2 * hid :, :] = dot(w[2 * hid :, :], s, 1, 1).astype(BF16)


def activation_body(parts, out):
    total = parts[0].astype(F32)
    for q in range(1, parts.shape[0]):
        total = total + parts[q].astype(F32)
    hid = total.shape[0] // 3
    gate, up, dhid = total[:hid], total[hid : 2 * hid], total[2 * hid :]
    sig = 1.0 / (1.0 + jnp.exp(-gate))
    active = gate * sig
    slope = sig * (1.0 + gate * (1.0 - sig))
    hidden = (active * up).astype(BF16)
    dgate = (dhid * up * slope).astype(BF16)
    dup = (dhid * active).astype(BF16)
    value = jnp.sum(hidden.astype(F32) * dhid, axis=0, keepdims=True)
    hi, lo = split_hi_lo(value)
    pad = jnp.zeros((out.shape[1] - 3 * hid - 2, out.shape[2]), BF16)
    block = jnp.concatenate([dgate, dup, hidden, hi, lo, pad], axis=0)
    for q in range(out.shape[0]):
        out[q] = block


def backward_body(here, acts, w0, w1, w2, w3, x_rows, s_rows, back, *grads):
    weights = (w0, w1, w2, w3)
    nx, ny = len(weights), back.shape[0]
    hid = w0.shape[0] // 3
    width = w0.shape[1]
    slots = acts.shape[2]
    terms = dot(w0[: 2 * hid, :], acts[here[0], : 2 * hid, :], 0, 0)
    for d in range(1, nx):
        q = (here[0] + nx - d) % nx
        terms = terms + dot(weights[d][: 2 * hid, :], acts[q, : 2 * hid, :], 0, 0)
    terms = terms.astype(BF16)
    x, s = x_rows[...], s_rows[...]
    norms = [jnp.zeros((1, width), F32) for _ in range(2)]
    value = jnp.zeros((1, slots), F32)
    for d in range(nx):
        q = (here[0] + d) % nx
        pair = dot(acts[q, : 2 * hid, :], x, 1, 0)
        down = dot(acts[q, 2 * hid : 3 * hid, :], s, 1, 0)
        grads[d][: 2 * hid, :] = pair.astype(BF16)
        grads[d][2 * hid :, :] = down.astype(BF16)
        for m in range(2):
            part = pair[m * hid : (m + 1) * hid]
            norms[m] = norms[m] + jnp.sum(part * part, axis=0, keepdims=True)
        tail = acts[q, 3 * hid : 3 * hid + 2, :].astype(F32)
        value = value + tail[0:1] + tail[1:2]
    flat = [v for n in norms for v in split_hi_lo(n)]
    lines = list(split_hi_lo(value))
    spare = (back.shape[1] - HALF - len(lines)) * slots - len(flat) * width
    flat = jnp.concatenate(flat + [jnp.zeros((1, spare), BF16)], axis=1)
    lines += [flat[:, k : k + slots] for k in range(0, flat.shape[1], slots)]
    extra = jnp.concatenate(lines, axis=0)
    for j in range(ny):
        back[j, :HALF, :] = terms[j * HALF : (j + 1) * HALF]
        back[j, HALF:, :] = extra


def gathered_body(parts, sent, norms):
    total = parts[0].astype(F32)
    for j in range(1, parts.shape[0]):
        total = total + parts[j].astype(F32)
    slots = total.shape[1]
    hi, lo = split_hi_lo(total[HALF : HALF + 1] + total[HALF + 1 : HALF + 2])
    pad = jnp.zeros((128 - HALF - 2, slots), F32)
    block = jnp.concatenate([total[:HALF], hi.astype(F32), lo.astype(F32), pad], axis=0)
    sent[...] = block.T.astype(BF16)
    flat = jnp.concatenate([total[k : k + 1] for k in range(HALF + 2, total.shape[0])], axis=1)
    tiles = [flat[:, k : k + 128] for k in range(0, flat.shape[1], 128)]
    each = norms.shape[0] // 2
    lines = [
        tiles[2 * m * each + k] + tiles[(2 * m + 1) * each + k]
        for m in range(2)
        for k in range(each)
    ]
    norms[...] = jnp.concatenate(lines, axis=0)


def halves(parts, lines, y, h):
    at = (y * HALF) % parts.shape[2]
    pair = [parts[2 * h + k, lines, at : at + HALF] for k in range(2)]
    return jnp.concatenate(pair, axis=1).astype(F32)


def grads_body(here, p0, p1, p2, p3, grad_gate, grad_up, grad_down, down_norms, parts):
    received = (p0, p1, p2, p3)
    nx = len(received)
    hid = grad_gate.shape[0]
    for d, p in enumerate(received):
        parts[(here[0] + nx - d) % nx] = p[...]
    acc = jnp.zeros((hid, 128), F32)
    for m, out in enumerate((grad_gate, grad_up, grad_down)):
        for y in range(parts.shape[2] // HALF):
            for h in range(nx // 2):
                tile = halves(parts, slice(m * hid, (m + 1) * hid), y, h)
                at = (y * (nx // 2) + h) * 128
                out[:, at : at + 128] = tile
                if m == 2:
                    acc = acc + tile * tile
    down_norms[...] = jnp.sum(acc.T, axis=0, keepdims=True)


def combine_body(
    here,
    back,
    positions,
    weights,
    n0,
    n1,
    n2,
    n3,
    grad_tokens,
    grad_route,
    gate_norms,
    up_norms,
    parts,
):
    slots, count = back.shape[0], positions.shape[1]
    pick = jnp.concatenate([chosen(positions[k : k + 1, :], slots) for k in range(2)], axis=1)
    got = dot(back[...], pick, 0, 0)
    grad_tokens[...] = (got[:HALF, :count] + got[:HALF, count:]).astype(BF16)
    value = got[HALF : HALF + 1] + got[HALF + 1 : HALF + 2]
    value = jnp.concatenate([value[:, :count], value[:, count:]], axis=0)
    grad_route[...] = value / weights[...]
    nx = parts.shape[0]
    for d, n in enumerate((n0, n1, n2, n3)):
        parts[(here[0] + nx - d) % nx] = n[...]
    each = n0.shape[0] // 2
    for m, out in enumerate((gate_norms, up_norms)):
        out[...] = jnp.concatenate(
            [
                halves(parts, slice(m * each + y // 2, m * each + y // 2 + 1), y, h)
                for y in range(2 * each)
                for h in range(nx // 2)
            ],
            axis=0,
        )


def call(body, outs, *args, fetch=False, far=False, scratch=()):
    smem = pl.BlockSpec(memory_space=pltpu.SMEM)
    vmem = pl.BlockSpec(memory_space=pltpu.VMEM)
    space = pltpu.HBM if fetch else pltpu.VMEM
    specs = [smem if a.ndim == 1 else pl.BlockSpec(memory_space=space) for a in args]
    args = [a if a.ndim == 1 else pltpu.with_memory_space_constraint(a, space) for a in args]
    shape = jax.ShapeDtypeStruct if far else pltpu.VMEM
    return pl.pallas_call(
        body,
        out_shape=[shape(s, d) for s, d in outs],
        in_specs=specs,
        out_specs=[vmem] * len(outs),
        scratch_shapes=list(scratch),
        compiler_params=pltpu.CompilerParams(vmem_limit_bytes=ROOM),
    )(*args)


def swap(a, axis):
    return lax.all_to_all(a, axis, 0, 0, tiled=True)


def shifted(pieces, axis):
    n = len(pieces)
    return [pieces[0]] + [
        lax.ppermute(pieces[d], axis, [(i, (i + d) % n) for i in range(n)])
        for d in range(1, n)
    ]


def layer(tokens, routes, route_weights, grad_out, w_gate, w_up, w_down):
    ny, nx = lax.axis_size("y"), lax.axis_size("x")
    sources = lax.axis_size("z") * lax.axis_size("c")
    here = lax.axis_index("x").astype(jnp.int32).reshape(1)
    count, feat = tokens.shape
    _, hid, width = w_gate.shape
    slots = sources * SLOTS
    quarter = width // nx
    small = [tokens.T, routes.T, route_weights.T, grad_out.T]
    sent, positions, scales = call(
        dispatch_body,
        [((slots, 2 * feat), BF16), ((2, count), jnp.int32), ((2, count), F32)],
        *small,
        fetch=True,
        scratch=[pltpu.VMEM(small[k].shape, small[k].dtype) for k in (0, 1, 3)]
        + [pltpu.SemaphoreType.DMA((4,))],
    )
    w_sent = call(
        quarter_weights_body,
        [((3 * hid, quarter), BF16)] * nx,
        here,
        w_gate[0],
        w_up[0],
        w_down[0],
        fetch=True,
        scratch=[pltpu.VMEM((hid, width), BF16)] * 3 + [pltpu.SemaphoreType.DMA((3,))],
    )
    weights = shifted(w_sent, "x")
    mine = swap(sent.reshape(sources, SLOTS, 2 * feat), ("z", "c"))
    mine = mine.reshape(slots, 2 * feat)
    (rows,) = call(copies_body, [((ny, slots, 2 * feat), BF16)], mine)
    rows = swap(rows, "y")
    parts, x_rows, s_rows = call(
        partial_body,
        [
            ((nx, 3 * hid, slots), BF16),
            ((slots, quarter), BF16),
            ((slots, quarter), BF16),
        ],
        here,
        rows,
        *weights,
    )
    parts = swap(parts, "x")
    (acts,) = call(activation_body, [((nx, 3 * hid + 8, slots), BF16)], parts)
    acts = swap(acts, "x")
    back, *grads = call(
        backward_body,
        [((ny, feat + 8, slots), BF16)] + [((3 * hid, quarter), BF16)] * nx,
        here,
        acts,
        *weights,
        x_rows,
        s_rows,
    )
    grads = shifted(grads, "x")
    back = swap(back, "y")
    back, grads = lax.optimization_barrier((back, grads))
    back_sent, norms = call(
        gathered_body, [((slots, 128), BF16), ((quarter // 64, 128), F32)], back
    )
    norms = shifted([norms] * nx, "x")
    back = swap(back_sent.reshape(sources, SLOTS, 128), ("z", "c"))
    back = back.reshape(slots, 128)
    grad_gate, grad_up, grad_down, down_norms = call(
        grads_body,
        [((hid, width), F32)] * 3 + [((1, hid), F32)],
        here,
        *grads,
        far=True,
        scratch=[pltpu.VMEM((nx, 3 * hid, quarter), BF16)],
    )
    grad_tokens, grad_route, gate_norms, up_norms = call(
        combine_body,
        [((feat, count), BF16), ((2, count), F32)] + [((width // 128, 128), F32)] * 2,
        here,
        back,
        positions,
        scales,
        *norms,
        far=True,
        scratch=[pltpu.VMEM((nx, quarter // 64, 128), F32)],
    )
    return (
        grad_tokens.T,
        grad_route.T,
        grad_gate[None],
        grad_up[None],
        grad_down[None],
        gate_norms.reshape(1, width),
        up_norms.reshape(1, width),
        down_norms,
    )


def solution(mesh):
    ep, tp = ("z", "c"), ("y", "x")
    fine = Mesh(mesh.devices.reshape(12, 2, 8, 4), ep + tp)
    in_specs = (
        P(ep, tp),
        P(ep, None),
        P(ep, None),
        P(ep, tp),
        P(ep, tp, None),
        P(ep, tp, None),
        P(ep, tp, None),
    )
    out_specs = (
        P(ep, tp),
        P(ep, None),
        P(ep, tp, None),
        P(ep, tp, None),
        P(ep, tp, None),
        P(ep, None),
        P(ep, None),
        P(ep, tp),
    )
    return jax.shard_map(layer, mesh=fine, in_specs=in_specs, out_specs=out_specs, check_vma=False)
```

```python
import jax
import jax.numpy as jnp
from jax import lax
from jax.experimental import pallas as pl
from jax.experimental.pallas import tpu as pltpu
from jax.sharding import Mesh
from jax.sharding import PartitionSpec as P


SLOTS = 16
HALF = 64
ROOM = 20 * 2**20
F32 = jnp.float32
BF16 = jnp.bfloat16


def dot(a, b, ca, cb):
    return lax.dot_general(a, b, (((ca,), (cb,)), ((), ())), preferred_element_type=F32)


def split_hi_lo(v):
    hi = v.astype(BF16)
    return hi, (v - hi.astype(F32)).astype(BF16)


def placed(routes, tokens, experts):
    ids = lax.broadcasted_iota(jnp.int32, (experts, tokens), 0)
    first = ids == routes[0:1, :]
    second = ids == routes[1:2, :]
    named = (first | second).astype(F32).astype(BF16)
    before = (
        lax.broadcasted_iota(jnp.int32, (tokens, tokens), 0)
        < lax.broadcasted_iota(jnp.int32, (tokens, tokens), 1)
    ).astype(F32).astype(BF16)
    rank = dot(named, before, 1, 0) + (ids * SLOTS).astype(F32)
    return [
        jnp.sum(jnp.where(m, rank, 0.0), axis=0, keepdims=True).astype(jnp.int32)
        for m in (first, second)
    ]


def chosen(position, slots):
    at = lax.broadcasted_iota(jnp.int32, (slots, position.shape[1]), 0)
    return (at == position).astype(F32).astype(BF16)


def fetched(sources, targets, sems):
    copies = [
        pltpu.make_async_copy(a, b, sems.at[k]) for k, (a, b) in enumerate(zip(sources, targets))
    ]
    for c in copies:
        c.start()
    return copies


def dispatch_body(
    tokens_far,
    routes_far,
    weights_far,
    cotangent_far,
    gate_far,
    up_far,
    down_far,
    sent,
    positions,
    weights,
    w_gate,
    w_up,
    w_down,
    tokens,
    routes,
    cotangent,
    sems,
    later_sems,
):
    far = (tokens_far, routes_far, weights_far, cotangent_far)
    now = fetched(far, (tokens, routes, weights, cotangent), sems)
    later = fetched((gate_far, up_far, down_far), (w_gate, w_up, w_down), later_sems)
    for c in now:
        c.wait()
    width, count = tokens.shape
    slots = sent.shape[0]
    at = placed(routes[...], count, slots // SLOTS)
    positions[...] = jnp.concatenate(at, axis=0)
    x = tokens[...]
    g = cotangent[...].astype(F32)
    scaled = [(g * weights[k : k + 1, :]).astype(BF16) for k in range(2)]
    rows = jnp.concatenate(
        [jnp.concatenate([x, x], axis=1), jnp.concatenate(scaled, axis=1)], axis=0
    )
    pick = jnp.concatenate([chosen(p, slots) for p in at], axis=1)
    sent[...] = dot(pick, rows, 1, 1).astype(BF16)
    for c in later:
        c.wait()


def quarter_weights_body(here, w_gate, w_up, w_down, o0, o1, o2, o3):
    outs = (o0, o1, o2, o3)
    nx = len(outs)
    hid = w_gate.shape[0]

    def write(at):
        for m, w in enumerate((w_gate, w_up, w_down)):
            for d, out in enumerate(outs):
                q = (at + d) % nx
                for j in range(out.shape[1] // 128):
                    a, b = ((2 * j) * nx + q) * HALF, ((2 * j + 1) * nx + q) * HALF
                    out[m * hid : (m + 1) * hid, j * 128 : (j + 1) * 128] = jnp.concatenate(
                        [w[:, a : a + HALF], w[:, b : b + HALF]], axis=1
                    )

    for at in range(nx):
        pl.when(here[0] == at)(lambda at=at: write(at))


def partial_body(here, rows, w0, w1, w2, w3, out, x_out, s_out):
    weights = (w0, w1, w2, w3)
    nx = len(weights)
    ny = rows.shape[0]
    for j in range(ny // 2):
        a, b = rows[2 * j], rows[2 * j + 1]
        x_out[:, j * 128 : (j + 1) * 128] = jnp.concatenate([a[:, :HALF], b[:, :HALF]], axis=1)
        s_out[:, j * 128 : (j + 1) * 128] = jnp.concatenate([a[:, HALF:], b[:, HALF:]], axis=1)
    x, s = x_out[...], s_out[...]
    hid = w0.shape[0] // 3
    both = dot(jnp.concatenate([w[: 2 * hid, :] for w in weights], axis=0), x, 1, 1)
    down = dot(jnp.concatenate([w[2 * hid :, :] for w in weights], axis=0), s, 1, 1)
    for d in range(nx):
        q = (here[0] + nx - d) % nx
        out[q, : 2 * hid, :] = both[2 * d * hid : 2 * (d + 1) * hid].astype(BF16)
        out[q, 2 * hid :, :] = down[d * hid : (d + 1) * hid].astype(BF16)


def activation_body(parts, out):
    total = parts[0].astype(F32)
    for q in range(1, parts.shape[0]):
        total = total + parts[q].astype(F32)
    hid = total.shape[0] // 3
    gate, up, dhid = total[:hid], total[hid : 2 * hid], total[2 * hid :]
    sig = 1.0 / (1.0 + jnp.exp(-gate))
    active = gate * sig
    slope = sig * (1.0 + gate * (1.0 - sig))
    hidden = (active * up).astype(BF16)
    dgate = (dhid * up * slope).astype(BF16)
    dup = (dhid * active).astype(BF16)
    value = jnp.sum(hidden.astype(F32) * dhid, axis=0, keepdims=True)
    hi, lo = split_hi_lo(value)
    pad = jnp.zeros((out.shape[1] - 3 * hid - 2, out.shape[2]), BF16)
    block = jnp.concatenate([dgate, dup, hidden, hi, lo, pad], axis=0)
    for q in range(out.shape[0]):
        out[q] = block


def backward_body(here, acts, w0, w1, w2, w3, x_rows, s_rows, back, *grads):
    weights = (w0, w1, w2, w3)
    nx, ny = len(weights), back.shape[0]
    hid = w0.shape[0] // 3
    width = w0.shape[1]
    slots = acts.shape[2]
    pairs = [acts[(here[0] + d) % nx, : 2 * hid, :] for d in range(nx)]
    terms = dot(
        jnp.concatenate([w[: 2 * hid, :] for w in weights], axis=0),
        jnp.concatenate([pairs[0]] + pairs[:0:-1], axis=0),
        0,
        0,
    ).astype(BF16)
    hiddens = [acts[(here[0] + d) % nx, 2 * hid : 3 * hid, :] for d in range(nx)]
    pair = dot(jnp.concatenate(pairs, axis=0), x_rows[...], 1, 0)
    down = dot(jnp.concatenate(hiddens, axis=0), s_rows[...], 1, 0)
    norms = [jnp.zeros((1, width), F32) for _ in range(2)]
    value = jnp.zeros((1, slots), F32)
    for d in range(nx):
        grads[d][: 2 * hid, :] = pair[2 * d * hid : 2 * (d + 1) * hid].astype(BF16)
        grads[d][2 * hid : 3 * hid, :] = down[d * hid : (d + 1) * hid].astype(BF16)
        for m in range(2):
            part = pair[(2 * d + m) * hid : (2 * d + m + 1) * hid]
            norms[m] = norms[m] + jnp.sum(part * part, axis=0, keepdims=True)
        tail = acts[(here[0] + d) % nx, 3 * hid : 3 * hid + 2, :].astype(F32)
        value = value + tail[0:1] + tail[1:2]
    flat = [v for n in norms for v in split_hi_lo(n)]
    lines = list(split_hi_lo(value))
    spare = (back.shape[1] - HALF - len(lines)) * slots - len(flat) * width
    flat = jnp.concatenate(flat + [jnp.zeros((1, spare), BF16)], axis=1)
    lines += [flat[:, k : k + slots] for k in range(0, flat.shape[1], slots)]
    extra = jnp.concatenate(lines, axis=0)
    for j in range(ny):
        back[j, :HALF, :] = terms[j * HALF : (j + 1) * HALF]
        back[j, HALF:, :] = extra


def gathered_body(parts, far, sent, norms, far_out):
    total = parts[0].astype(F32)
    for j in range(1, parts.shape[0]):
        total = total + parts[j].astype(F32)
    slots = total.shape[1]
    hi, lo = split_hi_lo(total[HALF : HALF + 1] + total[HALF + 1 : HALF + 2])
    pad = jnp.zeros((128 - HALF - 2, slots), F32)
    block = jnp.concatenate([total[:HALF], hi.astype(F32), lo.astype(F32), pad], axis=0)
    sent[...] = block.T.astype(BF16)
    flat = jnp.concatenate([total[k : k + 1] for k in range(HALF + 2, total.shape[0])], axis=1)
    tiles = [flat[:, k : k + 128] for k in range(0, flat.shape[1], 128)]
    each = norms.shape[0] // 2
    lines = [
        tiles[2 * m * each + k] + tiles[(2 * m + 1) * each + k]
        for m in range(2)
        for k in range(each)
    ]
    norms[...] = jnp.concatenate(lines, axis=0)
    both = [jnp.concatenate(lines[m * each : (m + 1) * each], axis=1) for m in range(2)]
    rows, width = far_out.shape
    tail = [v for n in both for v in split_hi_lo(n)] + [jnp.zeros((12, width), BF16)]
    far_out[rows - 16 :, :] = jnp.concatenate(tail, axis=0)


def halves(parts, lines, y, h):
    at = (y * HALF) % parts.shape[2]
    pair = [parts[2 * h + k, lines, at : at + HALF] for k in range(2)]
    return jnp.concatenate(pair, axis=1).astype(F32)


def grads_body(here, p0, p1, p2, p3, grad_gate, grad_up, grad_down, down_norms, parts):
    received = (p0, p1, p2, p3)
    nx = len(received)
    hid = grad_gate.shape[0]
    for d, p in enumerate(received):
        parts[(here[0] + nx - d) % nx] = p[: 3 * hid, :]
    acc = jnp.zeros((hid, 128), F32)
    for m, out in enumerate((grad_gate, grad_up, grad_down)):
        for y in range(parts.shape[2] // HALF):
            for h in range(nx // 2):
                tile = halves(parts, slice(m * hid, (m + 1) * hid), y, h)
                at = (y * (nx // 2) + h) * 128
                out[:, at : at + 128] = tile
                if m == 2:
                    acc = acc + tile * tile
    down_norms[...] = jnp.sum(acc.T, axis=0, keepdims=True)


def combine_body(
    here,
    back,
    positions,
    weights,
    n0,
    n1,
    far,
    n3,
    grad_tokens,
    grad_route,
    gate_norms,
    up_norms,
    parts,
):
    slots, count = back.shape[0], positions.shape[1]
    pick = jnp.concatenate([chosen(positions[k : k + 1, :], slots) for k in range(2)], axis=1)
    got = dot(back[...], pick, 0, 0)
    grad_tokens[...] = (got[:HALF, :count] + got[:HALF, count:]).astype(BF16)
    value = got[HALF : HALF + 1] + got[HALF + 1 : HALF + 2]
    value = jnp.concatenate([value[:, :count], value[:, count:]], axis=0)
    grad_route[...] = value / weights[...]
    nx = parts.shape[0]
    for d, n in ((0, n0), (1, n1), (3, n3)):
        parts[(here[0] + nx - d) % nx] = n[...]
    each = n0.shape[0] // 2
    tail = far[far.shape[0] - 16 :, :].astype(F32)
    both = [tail[2 * m : 2 * m + 1] + tail[2 * m + 1 : 2 * m + 2] for m in range(2)]
    parts[(here[0] + nx - 2) % nx] = jnp.concatenate(
        [v[:, k * 128 : (k + 1) * 128] for v in both for k in range(each)], axis=0
    )
    for m, out in enumerate((gate_norms, up_norms)):
        out[...] = jnp.concatenate(
            [
                halves(parts, slice(m * each + y // 2, m * each + y // 2 + 1), y, h)
                for y in range(2 * each)
                for h in range(nx // 2)
            ],
            axis=0,
        )


def call(body, outs, *args, name, fetch=False, far=False, scratch=(), aliases=None):
    smem = pl.BlockSpec(memory_space=pltpu.SMEM)
    vmem = pl.BlockSpec(memory_space=pltpu.VMEM)
    space = pltpu.HBM if fetch else pltpu.VMEM
    specs = [smem if a.ndim == 1 else pl.BlockSpec(memory_space=space) for a in args]
    args = [a if a.ndim == 1 else pltpu.with_memory_space_constraint(a, space) for a in args]
    shape = jax.ShapeDtypeStruct if far else pltpu.VMEM
    return pl.pallas_call(
        body,
        out_shape=[shape(s, d) for s, d in outs],
        in_specs=specs,
        out_specs=[vmem] * len(outs),
        scratch_shapes=list(scratch),
        input_output_aliases=aliases or {},
        compiler_params=pltpu.CompilerParams(vmem_limit_bytes=ROOM),
        name=name,
    )(*args)


def swap(a, axis):
    return lax.all_to_all(a, axis, 0, 0, tiled=True)


def shifted(piece, axis, d):
    n = lax.axis_size(axis)
    return lax.ppermute(piece, axis, [(i, (i + d) % n) for i in range(n)])


def per_device(tokens, routes, route_weights, grad_out, w_gate, w_up, w_down):
    ny, nx = lax.axis_size("y"), lax.axis_size("x")
    sources = lax.axis_size("z") * lax.axis_size("c")
    here = lax.axis_index("x").astype(jnp.int32).reshape(1)
    count, feat = tokens.shape
    _, hid, width = w_gate.shape
    slots = sources * SLOTS
    quarter = width // nx
    small = [tokens.T, routes.T, route_weights.T, grad_out.T]
    sent, positions, scales, *local = call(
        dispatch_body,
        [((slots, 2 * feat), BF16), ((2, count), jnp.int32), ((2, count), F32)]
        + [((hid, width), BF16)] * 3,
        *small,
        w_gate[0],
        w_up[0],
        w_down[0],
        name="dispatch",
        fetch=True,
        scratch=[pltpu.VMEM(small[k].shape, small[k].dtype) for k in (0, 1, 3)]
        + [pltpu.SemaphoreType.DMA((4,)), pltpu.SemaphoreType.DMA((3,))],
    )
    w_sent = call(
        quarter_weights_body,
        [((3 * hid, quarter), BF16)] * nx,
        here,
        *local,
        name="quarter_weights",
    )
    mine = swap(sent.reshape(sources, SLOTS, 2 * feat), ("z", "c")).reshape(slots, 2 * feat)
    weights = [w_sent[0]] + [shifted(w_sent[d], "x", d) for d in range(1, nx)]
    rows = lax.all_gather(mine, "y", axis=0, tiled=False)
    parts, x_rows, s_rows = call(
        partial_body,
        [
            ((nx, 3 * hid, slots), BF16),
            ((slots, quarter), BF16),
            ((slots, quarter), BF16),
        ],
        here,
        rows,
        *weights,
        name="partial",
    )
    parts = swap(parts, "x")
    (acts,) = call(
        activation_body, [((nx, 3 * hid + 8, slots), BF16)], parts, name="activation"
    )
    acts = swap(acts, "x")
    back, *grads = call(
        backward_body,
        [((ny, feat + 8, slots), BF16)]
        + [((3 * hid + (16 if d == 2 else 0), quarter), BF16) for d in range(nx)],
        here,
        acts,
        *weights,
        x_rows,
        s_rows,
        name="backward",
    )
    near = [shifted(grads[d], "x", d) for d in (1, 3)]
    back = swap(back, "y")
    back, near = lax.optimization_barrier((back, near))
    back_sent, norms, far = call(
        gathered_body,
        [
            ((slots, 128), BF16),
            ((quarter // 64, 128), F32),
            ((3 * hid + 16, quarter), BF16),
        ],
        back,
        grads[2],
        name="gathered",
        aliases={1: 2},
    )
    far = shifted(far, "x", 2)
    norms = [norms, shifted(norms, "x", 1), far, shifted(norms, "x", 3)]
    grads = [grads[0], near[0], far, near[1]]
    back = swap(back_sent.reshape(sources, SLOTS, 128), ("z", "c")).reshape(slots, 128)
    grad_gate, grad_up, grad_down, down_norms = call(
        grads_body,
        [((hid, width), F32)] * 3 + [((1, hid), F32)],
        here,
        *grads,
        name="grads",
        far=True,
        scratch=[pltpu.VMEM((nx, 3 * hid, quarter), BF16)],
    )
    grad_tokens, grad_route, gate_norms, up_norms = call(
        combine_body,
        [((feat, count), BF16), ((2, count), F32)] + [((width // 128, 128), F32)] * 2,
        here,
        back,
        positions,
        scales,
        *norms,
        name="combine",
        far=True,
        scratch=[pltpu.VMEM((nx, quarter // 64, 128), F32)],
    )
    return (
        grad_tokens.T,
        grad_route.T,
        grad_gate[None],
        grad_up[None],
        grad_down[None],
        gate_norms.reshape(1, width),
        up_norms.reshape(1, width),
        down_norms,
    )


def solution(mesh):
    ep, tp = ("z", "c"), ("y", "x")
    fine = Mesh(mesh.devices.reshape(12, 2, 8, 4), ep + tp)
    in_specs = (
        P(ep, tp),
        P(ep, None),
        P(ep, None),
        P(ep, tp),
        P(ep, tp, None),
        P(ep, tp, None),
        P(ep, tp, None),
    )
    out_specs = (
        P(ep, tp),
        P(ep, None),
        P(ep, tp, None),
        P(ep, tp, None),
        P(ep, tp, None),
        P(ep, None),
        P(ep, None),
        P(ep, tp),
    )
    return jax.shard_map(
        per_device, mesh=fine, in_specs=in_specs, out_specs=out_specs, check_vma=False
    )
```

```python
import jax
import jax.numpy as jnp
from jax import lax
from jax.experimental import pallas as pl
from jax.experimental.pallas import tpu as pltpu
from jax.sharding import Mesh
from jax.sharding import PartitionSpec as P


SLOTS = 16
HALF = 64
ROOM = 20 * 2**20
F32 = jnp.float32
BF16 = jnp.bfloat16


def dot(a, b, ca, cb):
    return lax.dot_general(a, b, (((ca,), (cb,)), ((), ())), preferred_element_type=F32)


def split_hi_lo(v):
    hi = v.astype(BF16)
    return hi, (v - hi.astype(F32)).astype(BF16)


def placed(routes, tokens, experts):
    ids = lax.broadcasted_iota(jnp.int32, (experts, tokens), 0)
    first = ids == routes[0:1, :]
    second = ids == routes[1:2, :]
    named = (first | second).astype(F32).astype(BF16)
    before = (
        lax.broadcasted_iota(jnp.int32, (tokens, tokens), 0)
        < lax.broadcasted_iota(jnp.int32, (tokens, tokens), 1)
    ).astype(F32).astype(BF16)
    rank = dot(named, before, 1, 0) + (ids * SLOTS).astype(F32)
    return [
        jnp.sum(jnp.where(m, rank, 0.0), axis=0, keepdims=True).astype(jnp.int32)
        for m in (first, second)
    ]


def chosen(position, slots):
    at = lax.broadcasted_iota(jnp.int32, (slots, position.shape[1]), 0)
    return (at == position).astype(F32).astype(BF16)


def fetched(sources, targets, sems):
    copies = [
        pltpu.make_async_copy(a, b, sems.at[k]) for k, (a, b) in enumerate(zip(sources, targets))
    ]
    for c in copies:
        c.start()
    return copies


def dispatch_body(
    tokens_far,
    routes_far,
    weights_far,
    cotangent_far,
    gate_far,
    up_far,
    down_far,
    sent,
    positions,
    weights,
    w_gate,
    w_up,
    w_down,
    tokens,
    routes,
    cotangent,
    sems,
    later_sems,
):
    far = (tokens_far, routes_far, weights_far, cotangent_far)
    now = fetched(far, (tokens, routes, weights, cotangent), sems)
    later = fetched((gate_far, up_far, down_far), (w_gate, w_up, w_down), later_sems)
    for c in now:
        c.wait()
    _, count = tokens.shape
    slots = sent.shape[0]
    at = placed(routes[...], count, slots // SLOTS)
    positions[...] = jnp.concatenate(at, axis=0)
    x = tokens[...]
    g = cotangent[...].astype(F32)
    scaled = [(g * weights[k : k + 1, :]).astype(BF16) for k in range(2)]
    rows = jnp.concatenate(
        [jnp.concatenate([x, x], axis=1), jnp.concatenate(scaled, axis=1)], axis=0
    )
    pick = jnp.concatenate([chosen(p, slots) for p in at], axis=1)
    sent[...] = dot(pick, rows, 1, 1).astype(BF16)
    for c in later:
        c.wait()


def quarter_weights_body(here, w_gate, w_up, w_down, o0, o1, o2, o3):
    outs = (o0, o1, o2, o3)
    nx = len(outs)
    hid = w_gate.shape[0]

    def write(at):
        for m, w in enumerate((w_gate, w_up, w_down)):
            for d, out in enumerate(outs):
                q = (at + d) % nx
                for j in range(out.shape[1] // 128):
                    a, b = ((2 * j) * nx + q) * HALF, ((2 * j + 1) * nx + q) * HALF
                    out[m * hid : (m + 1) * hid, j * 128 : (j + 1) * 128] = jnp.concatenate(
                        [w[:, a : a + HALF], w[:, b : b + HALF]], axis=1
                    )

    for at in range(nx):
        pl.when(here[0] == at)(lambda at=at: write(at))


def partial_body(here, rows, w0, w1, w2, w3, out, x_out, s_out):
    weights = (w0, w1, w2, w3)
    nx = len(weights)
    ny = rows.shape[0]
    for j in range(ny // 2):
        a, b = rows[2 * j], rows[2 * j + 1]
        x_out[:, j * 128 : (j + 1) * 128] = jnp.concatenate([a[:, :HALF], b[:, :HALF]], axis=1)
        s_out[:, j * 128 : (j + 1) * 128] = jnp.concatenate([a[:, HALF:], b[:, HALF:]], axis=1)
    x, s = x_out[...], s_out[...]
    hid = w0.shape[0] // 3
    both = dot(jnp.concatenate([w[: 2 * hid, :] for w in weights], axis=0), x, 1, 1)
    down = dot(jnp.concatenate([w[2 * hid :, :] for w in weights], axis=0), s, 1, 1)
    for d in range(nx):
        q = (here[0] + nx - d) % nx
        out[q, : 2 * hid, :] = both[2 * d * hid : 2 * (d + 1) * hid].astype(BF16)
        out[q, 2 * hid :, :] = down[d * hid : (d + 1) * hid].astype(BF16)


def activation_body(parts, out):
    total = parts[0].astype(F32)
    for q in range(1, parts.shape[0]):
        total = total + parts[q].astype(F32)
    hid = total.shape[0] // 3
    gate, up, dhid = total[:hid], total[hid : 2 * hid], total[2 * hid :]
    sig = 1.0 / (1.0 + jnp.exp(-gate))
    active = gate * sig
    slope = sig * (1.0 + gate * (1.0 - sig))
    hidden = (active * up).astype(BF16)
    dgate = (dhid * up * slope).astype(BF16)
    dup = (dhid * active).astype(BF16)
    value = jnp.sum(hidden.astype(F32) * dhid, axis=0, keepdims=True)
    hi, lo = split_hi_lo(value)
    pad = jnp.zeros((out.shape[1] - 3 * hid - 2, out.shape[2]), BF16)
    block = jnp.concatenate([dgate, dup, hidden, hi, lo, pad], axis=0)
    for q in range(out.shape[0]):
        out[q] = block


def backward_body(here, acts, w0, w1, w2, w3, x_rows, s_rows, back, *grads):
    weights = (w0, w1, w2, w3)
    nx, ny = len(weights), back.shape[0]
    hid = w0.shape[0] // 3
    width = w0.shape[1]
    slots = acts.shape[2]
    pairs = [acts[(here[0] + d) % nx, : 2 * hid, :] for d in range(nx)]
    terms = dot(
        jnp.concatenate([w[: 2 * hid, :] for w in weights], axis=0),
        jnp.concatenate([pairs[0]] + pairs[:0:-1], axis=0),
        0,
        0,
    ).astype(BF16)
    hiddens = [acts[(here[0] + d) % nx, 2 * hid : 3 * hid, :] for d in range(nx)]
    pair = dot(jnp.concatenate(pairs, axis=0), x_rows[...], 1, 0)
    down = dot(jnp.concatenate(hiddens, axis=0), s_rows[...], 1, 0)
    norms = [jnp.zeros((1, width), F32) for _ in range(2)]
    value = jnp.zeros((1, slots), F32)
    for d in range(nx):
        grads[d][: 2 * hid, :] = pair[2 * d * hid : 2 * (d + 1) * hid].astype(BF16)
        grads[d][2 * hid :, :] = down[d * hid : (d + 1) * hid].astype(BF16)
        for m in range(2):
            part = pair[(2 * d + m) * hid : (2 * d + m + 1) * hid]
            norms[m] = norms[m] + jnp.sum(part * part, axis=0, keepdims=True)
        tail = acts[(here[0] + d) % nx, 3 * hid : 3 * hid + 2, :].astype(F32)
        value = value + tail[0:1] + tail[1:2]
    flat = [v for n in norms for v in split_hi_lo(n)]
    lines = list(split_hi_lo(value))
    spare = (back.shape[1] - HALF - len(lines)) * slots - len(flat) * width
    flat = jnp.concatenate(flat + [jnp.zeros((1, spare), BF16)], axis=1)
    lines += [flat[:, k : k + slots] for k in range(0, flat.shape[1], slots)]
    extra = jnp.concatenate(lines, axis=0)
    for j in range(ny):
        back[j, :HALF, :] = terms[j * HALF : (j + 1) * HALF]
        back[j, HALF:, :] = extra


def gathered_body(parts, sent, norms):
    total = parts[0].astype(F32)
    for j in range(1, parts.shape[0]):
        total = total + parts[j].astype(F32)
    slots = total.shape[1]
    hi, lo = split_hi_lo(total[HALF : HALF + 1] + total[HALF + 1 : HALF + 2])
    pad = jnp.zeros((128 - HALF - 2, slots), F32)
    block = jnp.concatenate([total[:HALF], hi.astype(F32), lo.astype(F32), pad], axis=0)
    sent[...] = block.T.astype(BF16)
    flat = jnp.concatenate([total[k : k + 1] for k in range(HALF + 2, total.shape[0])], axis=1)
    tiles = [flat[:, k : k + 128] for k in range(0, flat.shape[1], 128)]
    each = norms.shape[0] // 2
    lines = [
        tiles[2 * m * each + k] + tiles[(2 * m + 1) * each + k]
        for m in range(2)
        for k in range(each)
    ]
    norms[...] = jnp.concatenate(lines, axis=0)


def halves(parts, lines, y, h):
    at = (y * HALF) % parts.shape[2]
    pair = [parts[2 * h + k, lines, at : at + HALF] for k in range(2)]
    return jnp.concatenate(pair, axis=1).astype(F32)


def grads_body(here, p0, p1, p2, p3, grad_gate, grad_up, grad_down, down_norms, parts):
    received = (p0, p1, p2, p3)
    nx = len(received)
    hid = grad_gate.shape[0]
    for d, p in enumerate(received):
        parts[(here[0] + nx - d) % nx] = p[...]
    acc = jnp.zeros((hid, 128), F32)
    for m, out in enumerate((grad_gate, grad_up, grad_down)):
        for y in range(parts.shape[2] // HALF):
            for h in range(nx // 2):
                tile = halves(parts, slice(m * hid, (m + 1) * hid), y, h)
                at = (y * (nx // 2) + h) * 128
                out[:, at : at + 128] = tile
                if m == 2:
                    acc = acc + tile * tile
    down_norms[...] = jnp.sum(acc.T, axis=0, keepdims=True)


def combine_body(
    here,
    back,
    positions,
    weights,
    n0,
    n1,
    n2,
    n3,
    grad_tokens,
    grad_route,
    gate_norms,
    up_norms,
    parts,
):
    slots, count = back.shape[0], positions.shape[1]
    pick = jnp.concatenate([chosen(positions[k : k + 1, :], slots) for k in range(2)], axis=1)
    got = dot(back[...], pick, 0, 0)
    grad_tokens[...] = (got[:HALF, :count] + got[:HALF, count:]).astype(BF16)
    value = got[HALF : HALF + 1] + got[HALF + 1 : HALF + 2]
    value = jnp.concatenate([value[:, :count], value[:, count:]], axis=0)
    grad_route[...] = value / weights[...]
    nx = parts.shape[0]
    each = parts.shape[1] // 2
    for d, n in enumerate((n0, n1, n2, n3)):
        parts[(here[0] + nx - d) % nx] = n[...]
    for m, out in enumerate((gate_norms, up_norms)):
        out[...] = jnp.concatenate(
            [
                halves(parts, slice(m * each + y // 2, m * each + y // 2 + 1), y, h)
                for y in range(2 * each)
                for h in range(nx // 2)
            ],
            axis=0,
        )


def call(body, outs, *args, fetch=False, far=False, scratch=(), aliases=None):
    smem = pl.BlockSpec(memory_space=pltpu.SMEM)
    vmem = pl.BlockSpec(memory_space=pltpu.VMEM)
    space = pltpu.HBM if fetch else pltpu.VMEM
    specs = [smem if a.ndim == 1 else pl.BlockSpec(memory_space=space) for a in args]
    args = [a if a.ndim == 1 else pltpu.with_memory_space_constraint(a, space) for a in args]
    shape = jax.ShapeDtypeStruct if far else pltpu.VMEM
    return pl.pallas_call(
        body,
        out_shape=[shape(s, d) for s, d in outs],
        in_specs=specs,
        out_specs=[vmem] * len(outs),
        scratch_shapes=list(scratch),
        input_output_aliases=aliases or {},
        compiler_params=pltpu.CompilerParams(vmem_limit_bytes=ROOM),
    )(*args)


def swap(a, axis):
    return lax.all_to_all(a, axis, 0, 0, tiled=True)


def shifted(piece, axis, d):
    n = lax.axis_size(axis)
    return lax.ppermute(piece, axis, [(i, (i + d) % n) for i in range(n)])


def layer(tokens, routes, route_weights, grad_out, w_gate, w_up, w_down):
    ny, nx = lax.axis_size("y"), lax.axis_size("x")
    sources = lax.axis_size("z") * lax.axis_size("c")
    here = lax.axis_index("x").astype(jnp.int32).reshape(1)
    count, feat = tokens.shape
    _, hid, width = w_gate.shape
    slots = sources * SLOTS
    quarter = width // nx
    small = [tokens.T, routes.T, route_weights.T, grad_out.T]
    sent, positions, scales, *local = call(
        dispatch_body,
        [((slots, 2 * feat), BF16), ((2, count), jnp.int32), ((2, count), F32)]
        + [((hid, width), BF16)] * 3,
        *small,
        w_gate[0],
        w_up[0],
        w_down[0],
        fetch=True,
        scratch=[pltpu.VMEM(small[k].shape, small[k].dtype) for k in (0, 1, 3)]
        + [pltpu.SemaphoreType.DMA((4,)), pltpu.SemaphoreType.DMA((3,))],
    )
    w_sent = call(quarter_weights_body, [((3 * hid, quarter), BF16)] * nx, here, *local)
    mine = swap(sent.reshape(sources, SLOTS, 2 * feat), ("z", "c")).reshape(slots, 2 * feat)
    weights = [w_sent[0]] + [shifted(w_sent[d], "x", d) for d in range(1, nx)]
    rows = lax.all_gather(mine, "y", axis=0, tiled=False)
    parts, x_rows, s_rows = call(
        partial_body,
        [
            ((nx, 3 * hid, slots), BF16),
            ((slots, quarter), BF16),
            ((slots, quarter), BF16),
        ],
        here,
        rows,
        *weights,
    )
    parts = swap(parts, "x")
    (acts,) = call(activation_body, [((nx, 3 * hid + 8, slots), BF16)], parts)
    acts = swap(acts, "x")
    back, *grads = call(
        backward_body,
        [((ny, feat + 8, slots), BF16)]
        + [((3 * hid, quarter), BF16)] * nx,
        here,
        acts,
        *weights,
        x_rows,
        s_rows,
    )
    grads = [grads[0]] + [shifted(grads[d], "x", d) for d in range(1, nx)]
    back = swap(back, "y")
    back, *grads[1::2] = lax.optimization_barrier((back, *grads[1::2]))
    back_sent, norms = call(
        gathered_body, [((slots, 128), BF16), ((quarter // 64, 128), F32)], back
    )
    norms = [norms] + [shifted(norms, "x", d) for d in range(1, nx)]
    back = swap(back_sent.reshape(sources, SLOTS, 128), ("z", "c")).reshape(slots, 128)
    grad_gate, grad_up, grad_down, down_norms = call(
        grads_body,
        [((hid, width), F32)] * 3 + [((1, hid), F32)],
        here,
        *grads,
        far=True,
        scratch=[pltpu.VMEM((nx, 3 * hid, quarter), BF16)],
    )
    grad_tokens, grad_route, gate_norms, up_norms = call(
        combine_body,
        [((feat, count), BF16), ((2, count), F32)] + [((width // 128, 128), F32)] * 2,
        here,
        back,
        positions,
        scales,
        *norms,
        far=True,
        scratch=[pltpu.VMEM((nx, quarter // 64, 128), F32)],
    )
    return (
        grad_tokens.T,
        grad_route.T,
        grad_gate[None],
        grad_up[None],
        grad_down[None],
        gate_norms.reshape(1, width),
        up_norms.reshape(1, width),
        down_norms,
    )


def solution(mesh):
    ep, tp = ("z", "c"), ("y", "x")
    fine = Mesh(mesh.devices.reshape(12, 2, 8, 4), ep + tp)
    in_specs = (
        P(ep, tp),
        P(ep, None),
        P(ep, None),
        P(ep, tp),
        P(ep, tp, None),
        P(ep, tp, None),
        P(ep, tp, None),
    )
    out_specs = (
        P(ep, tp),
        P(ep, None),
        P(ep, tp, None),
        P(ep, tp, None),
        P(ep, tp, None),
        P(ep, None),
        P(ep, None),
        P(ep, tp),
    )
    return jax.shard_map(layer, mesh=fine, in_specs=in_specs, out_specs=out_specs, check_vma=False)
```

```python
import jax
import jax.numpy as jnp
from jax import lax
from jax.experimental import pallas as pl
from jax.experimental.pallas import tpu as pltpu
from jax.sharding import Mesh
from jax.sharding import PartitionSpec as P


SLOTS = 16
HALF = 64
ROOM = 20 * 2**20
F32 = jnp.float32
BF16 = jnp.bfloat16


def dot(a, b, ca, cb):
    return lax.dot_general(a, b, (((ca,), (cb,)), ((), ())), preferred_element_type=F32)


def split_hi_lo(v):
    hi = v.astype(BF16)
    return hi, (v - hi.astype(F32)).astype(BF16)


def placed(routes, tokens, experts):
    ids = lax.broadcasted_iota(jnp.int32, (experts, tokens), 0)
    first = ids == routes[0:1, :]
    second = ids == routes[1:2, :]
    named = (first | second).astype(F32).astype(BF16)
    before = (
        lax.broadcasted_iota(jnp.int32, (tokens, tokens), 0)
        < lax.broadcasted_iota(jnp.int32, (tokens, tokens), 1)
    ).astype(F32).astype(BF16)
    rank = dot(named, before, 1, 0) + (ids * SLOTS).astype(F32)
    return [
        jnp.sum(jnp.where(m, rank, 0.0), axis=0, keepdims=True).astype(jnp.int32)
        for m in (first, second)
    ]


def chosen(position, slots):
    at = lax.broadcasted_iota(jnp.int32, (slots, position.shape[1]), 0)
    return (at == position).astype(F32).astype(BF16)


def fetched(sources, targets, sems):
    copies = [
        pltpu.make_async_copy(a, b, sems.at[k]) for k, (a, b) in enumerate(zip(sources, targets))
    ]
    for c in copies:
        c.start()
    return copies


def dispatch_body(
    tokens_far,
    routes_far,
    weights_far,
    cotangent_far,
    gate_far,
    up_far,
    down_far,
    sent,
    positions,
    weights,
    w_gate,
    w_up,
    w_down,
    tokens,
    routes,
    cotangent,
    sems,
    later_sems,
):
    far = (tokens_far, routes_far, weights_far, cotangent_far)
    now = fetched(far, (tokens, routes, weights, cotangent), sems)
    later = fetched((gate_far, up_far, down_far), (w_gate, w_up, w_down), later_sems)
    for c in now:
        c.wait()
    width, count = tokens.shape
    slots = sent.shape[0]
    at = placed(routes[...], count, slots // SLOTS)
    positions[...] = jnp.concatenate(at, axis=0)
    x = tokens[...]
    g = cotangent[...].astype(F32)
    scaled = [(g * weights[k : k + 1, :]).astype(BF16) for k in range(2)]
    rows = jnp.concatenate(
        [jnp.concatenate([x, x], axis=1), jnp.concatenate(scaled, axis=1)], axis=0
    )
    pick = jnp.concatenate([chosen(p, slots) for p in at], axis=1)
    sent[...] = dot(pick, rows, 1, 1).astype(BF16)
    for c in later:
        c.wait()


def quarter_weights_body(here, w_gate, w_up, w_down, o0, o1, o2, o3):
    outs = (o0, o1, o2, o3)
    nx = len(outs)
    hid = w_gate.shape[0]

    def write(at):
        for m, w in enumerate((w_gate, w_up, w_down)):
            for d, out in enumerate(outs):
                q = (at + d) % nx
                for j in range(out.shape[1] // 128):
                    a, b = ((2 * j) * nx + q) * HALF, ((2 * j + 1) * nx + q) * HALF
                    out[m * hid : (m + 1) * hid, j * 128 : (j + 1) * 128] = jnp.concatenate(
                        [w[:, a : a + HALF], w[:, b : b + HALF]], axis=1
                    )

    for at in range(nx):
        pl.when(here[0] == at)(lambda at=at: write(at))


def partial_body(here, rows, w0, w1, w2, w3, out, x_out, s_out):
    weights = (w0, w1, w2, w3)
    nx = len(weights)
    ny = rows.shape[1] // 128
    for j in range(ny // 2):
        a, b = (rows[:, k * 128 : (k + 1) * 128] for k in (2 * j, 2 * j + 1))
        x_out[:, j * 128 : (j + 1) * 128] = jnp.concatenate([a[:, :HALF], b[:, :HALF]], axis=1)
        s_out[:, j * 128 : (j + 1) * 128] = jnp.concatenate([a[:, HALF:], b[:, HALF:]], axis=1)
    x, s = x_out[...], s_out[...]
    hid = w0.shape[0] // 3
    both = dot(jnp.concatenate([w[: 2 * hid, :] for w in weights], axis=0), x, 1, 1)
    down = dot(jnp.concatenate([w[2 * hid :, :] for w in weights], axis=0), s, 1, 1)
    for d in range(nx):
        q = (here[0] + nx - d) % nx
        out[q, : 2 * hid, :] = both[2 * d * hid : 2 * (d + 1) * hid].astype(BF16)
        out[q, 2 * hid :, :] = down[d * hid : (d + 1) * hid].astype(BF16)


def activation_body(parts, out):
    total = parts[0].astype(F32)
    for q in range(1, parts.shape[0]):
        total = total + parts[q].astype(F32)
    hid = total.shape[0] // 3
    gate, up, dhid = total[:hid], total[hid : 2 * hid], total[2 * hid :]
    sig = 1.0 / (1.0 + jnp.exp(-gate))
    active = gate * sig
    slope = sig * (1.0 + gate * (1.0 - sig))
    hidden = (active * up).astype(BF16)
    dgate = (dhid * up * slope).astype(BF16)
    dup = (dhid * active).astype(BF16)
    value = jnp.sum(hidden.astype(F32) * dhid, axis=0, keepdims=True)
    hi, lo = split_hi_lo(value)
    pad = jnp.zeros((out.shape[1] - 3 * hid - 2, out.shape[2]), BF16)
    block = jnp.concatenate([dgate, dup, hidden, hi, lo, pad], axis=0)
    for q in range(out.shape[0]):
        out[q] = block


def backward_body(here, acts, w0, w1, w2, w3, x_rows, s_rows, back, *grads):
    weights = (w0, w1, w2, w3)
    nx, ny = len(weights), back.shape[0]
    hid = w0.shape[0] // 3
    width = w0.shape[1]
    slots = acts.shape[2]
    pairs = [acts[(here[0] + d) % nx, : 2 * hid, :] for d in range(nx)]
    terms = dot(
        jnp.concatenate([w[: 2 * hid, :] for w in weights], axis=0),
        jnp.concatenate([pairs[0]] + pairs[:0:-1], axis=0),
        0,
        0,
    ).astype(BF16)
    hiddens = [acts[(here[0] + d) % nx, 2 * hid : 3 * hid, :] for d in range(nx)]
    pair = dot(jnp.concatenate(pairs, axis=0), x_rows[...], 1, 0)
    down = dot(jnp.concatenate(hiddens, axis=0), s_rows[...], 1, 0)
    norms = [jnp.zeros((1, width), F32) for _ in range(2)]
    value = jnp.zeros((1, slots), F32)
    for d in range(nx):
        grads[d][: 2 * hid, :] = pair[2 * d * hid : 2 * (d + 1) * hid].astype(BF16)
        grads[d][2 * hid : 3 * hid, :] = down[d * hid : (d + 1) * hid].astype(BF16)
        for m in range(2):
            part = pair[(2 * d + m) * hid : (2 * d + m + 1) * hid]
            norms[m] = norms[m] + jnp.sum(part * part, axis=0, keepdims=True)
        tail = acts[(here[0] + d) % nx, 3 * hid : 3 * hid + 2, :].astype(F32)
        value = value + tail[0:1] + tail[1:2]
    flat = [v for n in norms for v in split_hi_lo(n)]
    lines = list(split_hi_lo(value))
    spare = (back.shape[1] - HALF - len(lines)) * slots - len(flat) * width
    flat = jnp.concatenate(flat + [jnp.zeros((1, spare), BF16)], axis=1)
    lines += [flat[:, k : k + slots] for k in range(0, flat.shape[1], slots)]
    extra = jnp.concatenate(lines, axis=0)
    for j in range(ny):
        back[j, :HALF, :] = terms[j * HALF : (j + 1) * HALF]
        back[j, HALF:, :] = extra


def gathered_body(parts, far, sent, norms, far_out):
    total = parts[0].astype(F32)
    for j in range(1, parts.shape[0]):
        total = total + parts[j].astype(F32)
    slots = total.shape[1]
    hi, lo = split_hi_lo(total[HALF : HALF + 1] + total[HALF + 1 : HALF + 2])
    pad = jnp.zeros((128 - HALF - 2, slots), F32)
    block = jnp.concatenate([total[:HALF], hi.astype(F32), lo.astype(F32), pad], axis=0)
    sent[...] = block.T.astype(BF16)
    flat = jnp.concatenate([total[k : k + 1] for k in range(HALF + 2, total.shape[0])], axis=1)
    tiles = [flat[:, k : k + 128] for k in range(0, flat.shape[1], 128)]
    each = norms.shape[0] // 2
    lines = [
        tiles[2 * m * each + k] + tiles[(2 * m + 1) * each + k]
        for m in range(2)
        for k in range(each)
    ]
    norms[...] = jnp.concatenate(lines, axis=0)
    both = [jnp.concatenate(lines[m * each : (m + 1) * each], axis=1) for m in range(2)]
    rows, width = far_out.shape
    tail = [v for n in both for v in split_hi_lo(n)] + [jnp.zeros((12, width), BF16)]
    far_out[rows - 16 :, :] = jnp.concatenate(tail, axis=0)


def halves(parts, lines, y, h):
    at = (y * HALF) % parts.shape[2]
    pair = [parts[2 * h + k, lines, at : at + HALF] for k in range(2)]
    return jnp.concatenate(pair, axis=1).astype(F32)


def grads_body(here, p0, p1, p2, p3, grad_gate, grad_up, grad_down, down_norms, parts):
    received = (p0, p1, p2, p3)
    nx = len(received)
    hid = grad_gate.shape[0]
    for d, p in enumerate(received):
        parts[(here[0] + nx - d) % nx] = p[: 3 * hid, :]
    acc = jnp.zeros((hid, 128), F32)
    for m, out in enumerate((grad_gate, grad_up, grad_down)):
        for y in range(parts.shape[2] // HALF):
            for h in range(nx // 2):
                tile = halves(parts, slice(m * hid, (m + 1) * hid), y, h)
                at = (y * (nx // 2) + h) * 128
                out[:, at : at + 128] = tile
                if m == 2:
                    acc = acc + tile * tile
    down_norms[...] = jnp.sum(acc.T, axis=0, keepdims=True)


def combine_body(
    here,
    back,
    positions,
    weights,
    n0,
    n1,
    far,
    n3,
    grad_tokens,
    grad_route,
    gate_norms,
    up_norms,
    parts,
):
    slots, count = back.shape[0], positions.shape[1]
    pick = jnp.concatenate([chosen(positions[k : k + 1, :], slots) for k in range(2)], axis=1)
    got = dot(back[...], pick, 0, 0)
    grad_tokens[...] = (got[:HALF, :count] + got[:HALF, count:]).astype(BF16)
    value = got[HALF : HALF + 1] + got[HALF + 1 : HALF + 2]
    value = jnp.concatenate([value[:, :count], value[:, count:]], axis=0)
    grad_route[...] = value / weights[...]
    nx = parts.shape[0]
    for d, n in ((0, n0), (1, n1), (3, n3)):
        parts[(here[0] + nx - d) % nx] = n[...]
    each = n0.shape[0] // 2
    tail = far[far.shape[0] - 16 :, :].astype(F32)
    both = [tail[2 * m : 2 * m + 1] + tail[2 * m + 1 : 2 * m + 2] for m in range(2)]
    parts[(here[0] + nx - 2) % nx] = jnp.concatenate(
        [v[:, k * 128 : (k + 1) * 128] for v in both for k in range(each)], axis=0
    )
    for m, out in enumerate((gate_norms, up_norms)):
        out[...] = jnp.concatenate(
            [
                halves(parts, slice(m * each + y // 2, m * each + y // 2 + 1), y, h)
                for y in range(2 * each)
                for h in range(nx // 2)
            ],
            axis=0,
        )


def call(body, outs, *args, name, fetch=False, far=False, scratch=(), aliases=None):
    smem = pl.BlockSpec(memory_space=pltpu.SMEM)
    vmem = pl.BlockSpec(memory_space=pltpu.VMEM)
    space = pltpu.HBM if fetch else pltpu.VMEM
    specs = [smem if a.ndim == 1 else pl.BlockSpec(memory_space=space) for a in args]
    args = [a if a.ndim == 1 else pltpu.with_memory_space_constraint(a, space) for a in args]
    shape = jax.ShapeDtypeStruct if far else pltpu.VMEM
    return pl.pallas_call(
        body,
        out_shape=[shape(s, d) for s, d in outs],
        in_specs=specs,
        out_specs=[vmem] * len(outs),
        scratch_shapes=list(scratch),
        input_output_aliases=aliases or {},
        compiler_params=pltpu.CompilerParams(vmem_limit_bytes=ROOM),
        name=name,
    )(*args)


def swap(a, axis):
    return lax.all_to_all(a, axis, 0, 0, tiled=True)


def shifted(piece, axis, d):
    n = lax.axis_size(axis)
    return lax.ppermute(piece, axis, [(i, (i + d) % n) for i in range(n)])


def per_device(tokens, routes, route_weights, grad_out, w_gate, w_up, w_down):
    ny, nx = lax.axis_size("y"), lax.axis_size("x")
    sources = lax.axis_size("z") * lax.axis_size("c")
    here = lax.axis_index("x").astype(jnp.int32).reshape(1)
    count, feat = tokens.shape
    _, hid, width = w_gate.shape
    slots = sources * SLOTS
    quarter = width // nx
    small = [tokens.T, routes.T, route_weights.T, grad_out.T]
    sent, positions, scales, *local = call(
        dispatch_body,
        [((slots, 2 * feat), BF16), ((2, count), jnp.int32), ((2, count), F32)]
        + [((hid, width), BF16)] * 3,
        *small,
        w_gate[0],
        w_up[0],
        w_down[0],
        name="dispatch",
        fetch=True,
        scratch=[pltpu.VMEM(small[k].shape, small[k].dtype) for k in (0, 1, 3)]
        + [pltpu.SemaphoreType.DMA((4,)), pltpu.SemaphoreType.DMA((3,))],
    )
    w_sent = call(
        quarter_weights_body,
        [((3 * hid, quarter), BF16)] * nx,
        here,
        *local,
        name="quarter_weights",
    )
    mine = swap(sent.reshape(sources, SLOTS, 2 * feat), ("z", "c")).reshape(slots, 2 * feat)
    weights = [w_sent[0]] + [shifted(w_sent[d], "x", d) for d in range(1, nx)]
    rows = lax.all_gather(mine, "y", axis=1, tiled=True)
    parts, x_rows, s_rows = call(
        partial_body,
        [
            ((nx, 3 * hid, slots), BF16),
            ((slots, quarter), BF16),
            ((slots, quarter), BF16),
        ],
        here,
        rows,
        *weights,
        name="partial",
    )
    parts = swap(parts, "x")
    (acts,) = call(
        activation_body, [((nx, 3 * hid + 8, slots), BF16)], parts, name="activation"
    )
    acts = swap(acts, "x")
    back, *grads = call(
        backward_body,
        [((ny, feat + 8, slots), BF16)]
        + [((3 * hid + (16 if d == 2 else 0), quarter), BF16) for d in range(nx)],
        here,
        acts,
        *weights,
        x_rows,
        s_rows,
        name="backward",
    )
    near = [shifted(grads[d], "x", d) for d in (1, 3)]
    back = swap(back, "y")
    back, near = lax.optimization_barrier((back, near))
    back_sent, norms, far = call(
        gathered_body,
        [
            ((slots, 128), BF16),
            ((quarter // 64, 128), F32),
            ((3 * hid + 16, quarter), BF16),
        ],
        back,
        grads[2],
        name="gathered",
        aliases={1: 2},
    )
    far = shifted(far, "x", 2)
    norms = [norms, shifted(norms, "x", 1), far, shifted(norms, "x", 3)]
    grads = [grads[0], near[0], far, near[1]]
    back = swap(back_sent.reshape(sources, SLOTS, 128), ("z", "c")).reshape(slots, 128)
    grad_gate, grad_up, grad_down, down_norms = call(
        grads_body,
        [((hid, width), F32)] * 3 + [((1, hid), F32)],
        here,
        *grads,
        name="grads",
        far=True,
        scratch=[pltpu.VMEM((nx, 3 * hid, quarter), BF16)],
    )
    grad_tokens, grad_route, gate_norms, up_norms = call(
        combine_body,
        [((feat, count), BF16), ((2, count), F32)] + [((width // 128, 128), F32)] * 2,
        here,
        back,
        positions,
        scales,
        *norms,
        name="combine",
        far=True,
        scratch=[pltpu.VMEM((nx, quarter // 64, 128), F32)],
    )
    return (
        grad_tokens.T,
        grad_route.T,
        grad_gate[None],
        grad_up[None],
        grad_down[None],
        gate_norms.reshape(1, width),
        up_norms.reshape(1, width),
        down_norms,
    )


def solution(mesh):
    ep, tp = ("z", "c"), ("y", "x")
    fine = Mesh(mesh.devices.reshape(12, 2, 8, 4), ep + tp)
    in_specs = (
        P(ep, tp),
        P(ep, None),
        P(ep, None),
        P(ep, tp),
        P(ep, tp, None),
        P(ep, tp, None),
        P(ep, tp, None),
    )
    out_specs = (
        P(ep, tp),
        P(ep, None),
        P(ep, tp, None),
        P(ep, tp, None),
        P(ep, tp, None),
        P(ep, None),
        P(ep, None),
        P(ep, tp),
    )
    return jax.shard_map(
        per_device, mesh=fine, in_specs=in_specs, out_specs=out_specs, check_vma=False
    )
```

```python
import jax
import jax.numpy as jnp
from jax import lax
from jax.experimental import pallas as pl
from jax.experimental.pallas import tpu as pltpu
from jax.sharding import Mesh
from jax.sharding import PartitionSpec as P


SLOTS = 16
HALF = 64
ROOM = 20 * 2**20
F32 = jnp.float32
BF16 = jnp.bfloat16


def dot(a, b, ca, cb):
    return lax.dot_general(a, b, (((ca,), (cb,)), ((), ())), preferred_element_type=F32)


def split_hi_lo(v):
    hi = v.astype(BF16)
    return hi, (v - hi.astype(F32)).astype(BF16)


def placed(routes, tokens, experts):
    ids = lax.broadcasted_iota(jnp.int32, (experts, tokens), 0)
    first = ids == routes[0:1, :]
    second = ids == routes[1:2, :]
    named = (first | second).astype(F32).astype(BF16)
    before = (
        lax.broadcasted_iota(jnp.int32, (tokens, tokens), 0)
        < lax.broadcasted_iota(jnp.int32, (tokens, tokens), 1)
    ).astype(F32).astype(BF16)
    rank = dot(named, before, 1, 0) + (ids * SLOTS).astype(F32)
    return [
        jnp.sum(jnp.where(m, rank, 0.0), axis=0, keepdims=True).astype(jnp.int32)
        for m in (first, second)
    ]


def chosen(position, slots):
    at = lax.broadcasted_iota(jnp.int32, (slots, position.shape[1]), 0)
    return (at == position).astype(F32).astype(BF16)


def fetched(sources, targets, sems):
    copies = [
        pltpu.make_async_copy(a, b, sems.at[k]) for k, (a, b) in enumerate(zip(sources, targets))
    ]
    for c in copies:
        c.start()
    return copies


def dispatch_body(
    tokens_far,
    routes_far,
    weights_far,
    cotangent_far,
    gate_far,
    up_far,
    down_far,
    sent,
    positions,
    weights,
    w_gate,
    w_up,
    w_down,
    tokens,
    routes,
    cotangent,
    sems,
    later_sems,
):
    far = (tokens_far, routes_far, weights_far, cotangent_far)
    now = fetched(far, (tokens, routes, weights, cotangent), sems)
    later = fetched((gate_far, up_far, down_far), (w_gate, w_up, w_down), later_sems)
    for c in now:
        c.wait()
    _, count = tokens.shape
    slots = sent.shape[0]
    at = placed(routes[...], count, slots // SLOTS)
    positions[...] = jnp.concatenate(at, axis=0)
    x = tokens[...]
    g = cotangent[...].astype(F32)
    scaled = [(g * weights[k : k + 1, :]).astype(BF16) for k in range(2)]
    rows = jnp.concatenate(
        [jnp.concatenate([x, x], axis=1), jnp.concatenate(scaled, axis=1)], axis=0
    )
    pick = jnp.concatenate([chosen(p, slots) for p in at], axis=1)
    sent[...] = dot(pick, rows, 1, 1).astype(BF16)
    for c in later:
        c.wait()


def quarter_weights_body(here, w_gate, w_up, w_down, o0, o1, o2, o3):
    outs = (o0, o1, o2, o3)
    nx = len(outs)
    hid = w_gate.shape[0]

    def write(at):
        for m, w in enumerate((w_gate, w_up, w_down)):
            for d, out in enumerate(outs):
                q = (at + d) % nx
                for j in range(out.shape[1] // 128):
                    a, b = ((2 * j) * nx + q) * HALF, ((2 * j + 1) * nx + q) * HALF
                    out[m * hid : (m + 1) * hid, j * 128 : (j + 1) * 128] = jnp.concatenate(
                        [w[:, a : a + HALF], w[:, b : b + HALF]], axis=1
                    )

    for at in range(nx):
        pl.when(here[0] == at)(lambda at=at: write(at))


def partial_body(here, rows, w0, w1, w2, w3, out, x_out, s_out):
    weights = (w0, w1, w2, w3)
    nx = len(weights)
    ny = rows.shape[1] // 128
    for j in range(ny // 2):
        a, b = (rows[:, k * 128 : (k + 1) * 128] for k in (2 * j, 2 * j + 1))
        x_out[:, j * 128 : (j + 1) * 128] = jnp.concatenate([a[:, :HALF], b[:, :HALF]], axis=1)
        s_out[:, j * 128 : (j + 1) * 128] = jnp.concatenate([a[:, HALF:], b[:, HALF:]], axis=1)
    x, s = x_out[...], s_out[...]
    hid = w0.shape[0] // 3
    both = dot(jnp.concatenate([w[: 2 * hid, :] for w in weights], axis=0), x, 1, 1)
    down = dot(jnp.concatenate([w[2 * hid :, :] for w in weights], axis=0), s, 1, 1)
    for d in range(nx):
        q = (here[0] + nx - d) % nx
        out[q, : 2 * hid, :] = both[2 * d * hid : 2 * (d + 1) * hid].astype(BF16)
        out[q, 2 * hid :, :] = down[d * hid : (d + 1) * hid].astype(BF16)


def activation_body(parts, out):
    total = parts[0].astype(F32)
    for q in range(1, parts.shape[0]):
        total = total + parts[q].astype(F32)
    hid = total.shape[0] // 3
    gate, up, dhid = total[:hid], total[hid : 2 * hid], total[2 * hid :]
    sig = 1.0 / (1.0 + jnp.exp(-gate))
    active = gate * sig
    slope = sig * (1.0 + gate * (1.0 - sig))
    hidden = (active * up).astype(BF16)
    dgate = (dhid * up * slope).astype(BF16)
    dup = (dhid * active).astype(BF16)
    value = jnp.sum(hidden.astype(F32) * dhid, axis=0, keepdims=True)
    hi, lo = split_hi_lo(value)
    pad = jnp.zeros((out.shape[1] - 3 * hid - 2, out.shape[2]), BF16)
    block = jnp.concatenate([dgate, dup, hidden, hi, lo, pad], axis=0)
    for q in range(out.shape[0]):
        out[q] = block


def backward_body(
    here, acts, w0, w1, w2, w3, x_rows, s_rows, back_far, g0, g1, g2, g3, back, sems
):
    weights = (w0, w1, w2, w3)
    grads = (g0, g1, g2, g3)
    nx, ny = len(weights), back.shape[0]
    hid = w0.shape[0] // 3
    width = w0.shape[1]
    slots = acts.shape[2]
    pairs = [acts[(here[0] + d) % nx, : 2 * hid, :] for d in range(nx)]
    terms = dot(
        jnp.concatenate([w[: 2 * hid, :] for w in weights], axis=0),
        jnp.concatenate([pairs[0]] + pairs[:0:-1], axis=0),
        0,
        0,
    ).astype(BF16)
    for j in range(ny):
        back[j, :HALF, :] = terms[j * HALF : (j + 1) * HALF]
    ends = (slice(0, HALF), slice(HALF, back.shape[1]))
    out_copies = [
        pltpu.make_async_copy(back.at[:, e, :], back_far.at[:, e, :], sems.at[k])
        for k, e in enumerate(ends)
    ]
    out_copies[0].start()
    hiddens = [acts[(here[0] + d) % nx, 2 * hid : 3 * hid, :] for d in range(nx)]
    pair = dot(jnp.concatenate(pairs, axis=0), x_rows[...], 1, 0)
    down = dot(jnp.concatenate(hiddens, axis=0), s_rows[...], 1, 0)
    norms = [jnp.zeros((1, width), F32) for _ in range(2)]
    value = jnp.zeros((1, slots), F32)
    for d in range(nx):
        grads[d][: 2 * hid, :] = pair[2 * d * hid : 2 * (d + 1) * hid].astype(BF16)
        grads[d][2 * hid :, :] = down[d * hid : (d + 1) * hid].astype(BF16)
        for m in range(2):
            part = pair[(2 * d + m) * hid : (2 * d + m + 1) * hid]
            norms[m] = norms[m] + jnp.sum(part * part, axis=0, keepdims=True)
        tail = acts[(here[0] + d) % nx, 3 * hid : 3 * hid + 2, :].astype(F32)
        value = value + tail[0:1] + tail[1:2]
    flat = [v for n in norms for v in split_hi_lo(n)]
    lines = list(split_hi_lo(value))
    spare = (back.shape[1] - HALF - len(lines)) * slots - len(flat) * width
    flat = jnp.concatenate(flat + [jnp.zeros((1, spare), BF16)], axis=1)
    lines += [flat[:, k : k + slots] for k in range(0, flat.shape[1], slots)]
    extra = jnp.concatenate(lines, axis=0)
    for j in range(ny):
        back[j, HALF:, :] = extra
    out_copies[1].start()
    for c in out_copies:
        c.wait()


def gathered_body(parts, sent, norms):
    total = parts[0].astype(F32)
    for j in range(1, parts.shape[0]):
        total = total + parts[j].astype(F32)
    slots = total.shape[1]
    hi, lo = split_hi_lo(total[HALF : HALF + 1] + total[HALF + 1 : HALF + 2])
    pad = jnp.zeros((128 - HALF - 2, slots), F32)
    block = jnp.concatenate([total[:HALF], hi.astype(F32), lo.astype(F32), pad], axis=0)
    sent[...] = block.T.astype(BF16)
    flat = jnp.concatenate([total[k : k + 1] for k in range(HALF + 2, total.shape[0])], axis=1)
    tiles = [flat[:, k : k + 128] for k in range(0, flat.shape[1], 128)]
    each = norms.shape[0] // 2
    lines = [
        tiles[2 * m * each + k] + tiles[(2 * m + 1) * each + k]
        for m in range(2)
        for k in range(each)
    ]
    norms[...] = jnp.concatenate(lines, axis=0)


def halves(parts, lines, y, h):
    at = (y * HALF) % parts.shape[2]
    pair = [parts[2 * h + k, lines, at : at + HALF] for k in range(2)]
    return jnp.concatenate(pair, axis=1).astype(F32)


def grads_body(here, p0, p1, p2, p3, grad_gate, grad_up, grad_down, down_norms, parts):
    received = (p0, p1, p2, p3)
    nx = len(received)
    hid = grad_gate.shape[0]
    for d, p in enumerate(received):
        parts[(here[0] + nx - d) % nx] = p[...]
    acc = jnp.zeros((hid, 128), F32)
    for m, out in enumerate((grad_gate, grad_up, grad_down)):
        for y in range(parts.shape[2] // HALF):
            for h in range(nx // 2):
                tile = halves(parts, slice(m * hid, (m + 1) * hid), y, h)
                at = (y * (nx // 2) + h) * 128
                out[:, at : at + 128] = tile
                if m == 2:
                    acc = acc + tile * tile
    down_norms[...] = jnp.sum(acc.T, axis=0, keepdims=True)


def combine_body(
    here,
    back,
    positions,
    weights,
    n0,
    n1,
    n2,
    n3,
    grad_tokens,
    grad_route,
    gate_norms,
    up_norms,
    parts,
):
    slots, count = back.shape[0], positions.shape[1]
    pick = jnp.concatenate([chosen(positions[k : k + 1, :], slots) for k in range(2)], axis=1)
    got = dot(back[...], pick, 0, 0)
    grad_tokens[...] = (got[:HALF, :count] + got[:HALF, count:]).astype(BF16)
    value = got[HALF : HALF + 1] + got[HALF + 1 : HALF + 2]
    value = jnp.concatenate([value[:, :count], value[:, count:]], axis=0)
    grad_route[...] = value / weights[...]
    nx = parts.shape[0]
    each = parts.shape[1] // 2
    for d, n in enumerate((n0, n1, n2, n3)):
        parts[(here[0] + nx - d) % nx] = n[...]
    for m, out in enumerate((gate_norms, up_norms)):
        out[...] = jnp.concatenate(
            [
                halves(parts, slice(m * each + y // 2, m * each + y // 2 + 1), y, h)
                for y in range(2 * each)
                for h in range(nx // 2)
            ],
            axis=0,
        )


def call(body, outs, *args, fetch=False, far=False, scratch=(), aliases=None, sent=()):
    smem = pl.BlockSpec(memory_space=pltpu.SMEM)
    vmem = pl.BlockSpec(memory_space=pltpu.VMEM)
    space = pltpu.HBM if fetch else pltpu.VMEM
    specs = [smem if a.ndim == 1 else pl.BlockSpec(memory_space=space) for a in args]
    args = [a if a.ndim == 1 else pltpu.with_memory_space_constraint(a, space) for a in args]
    shape = jax.ShapeDtypeStruct if far else pltpu.VMEM
    shapes = [pltpu.HBM(a, d) if k in sent else shape(a, d) for k, (a, d) in enumerate(outs)]
    return pl.pallas_call(
        body,
        out_shape=shapes,
        in_specs=specs,
        out_specs=[
            pl.BlockSpec(memory_space=pltpu.HBM) if k in sent else vmem for k in range(len(outs))
        ],
        scratch_shapes=list(scratch),
        input_output_aliases=aliases or {},
        compiler_params=pltpu.CompilerParams(vmem_limit_bytes=ROOM),
    )(*args)


def swap(a, axis):
    return lax.all_to_all(a, axis, 0, 0, tiled=True)


def shifted(piece, axis, d):
    n = lax.axis_size(axis)
    return lax.ppermute(piece, axis, [(i, (i + d) % n) for i in range(n)])


def layer(tokens, routes, route_weights, grad_out, w_gate, w_up, w_down):
    ny, nx = lax.axis_size("y"), lax.axis_size("x")
    sources = lax.axis_size("z") * lax.axis_size("c")
    here = lax.axis_index("x").astype(jnp.int32).reshape(1)
    count, feat = tokens.shape
    _, hid, width = w_gate.shape
    slots = sources * SLOTS
    quarter = width // nx
    small = [tokens.T, routes.T, route_weights.T, grad_out.T]
    sent, positions, scales, *local = call(
        dispatch_body,
        [((slots, 2 * feat), BF16), ((2, count), jnp.int32), ((2, count), F32)]
        + [((hid, width), BF16)] * 3,
        *small,
        w_gate[0],
        w_up[0],
        w_down[0],
        fetch=True,
        scratch=[pltpu.VMEM(small[k].shape, small[k].dtype) for k in (0, 1, 3)]
        + [pltpu.SemaphoreType.DMA((4,)), pltpu.SemaphoreType.DMA((3,))],
    )
    w_sent = call(quarter_weights_body, [((3 * hid, quarter), BF16)] * nx, here, *local)
    mine = swap(sent.reshape(sources, SLOTS, 2 * feat), ("z", "c")).reshape(slots, 2 * feat)
    weights = [w_sent[0]] + [shifted(w_sent[d], "x", d) for d in range(1, nx)]
    rows = lax.all_gather(mine, "y", axis=1, tiled=True)
    parts, x_rows, s_rows = call(
        partial_body,
        [
            ((nx, 3 * hid, slots), BF16),
            ((slots, quarter), BF16),
            ((slots, quarter), BF16),
        ],
        here,
        rows,
        *weights,
    )
    parts = swap(parts, "x")
    (acts,) = call(activation_body, [((nx, 3 * hid + 8, slots), BF16)], parts)
    acts = swap(acts, "x")
    back, *grads = call(
        backward_body,
        [((ny, feat + 8, slots), BF16)]
        + [((3 * hid, quarter), BF16)] * nx,
        here,
        acts,
        *weights,
        x_rows,
        s_rows,
        sent=(0,),
        scratch=[pltpu.VMEM((ny, feat + 8, slots), BF16), pltpu.SemaphoreType.DMA((2,))],
    )
    grads = [grads[0]] + [shifted(grads[d], "x", d) for d in range(1, nx)]
    back = swap(back, "y")
    back, *grads[1::2] = lax.optimization_barrier((back, *grads[1::2]))
    back_sent, norms = call(
        gathered_body, [((slots, 128), BF16), ((quarter // 64, 128), F32)], back
    )
    norms = [norms] + [shifted(norms, "x", d) for d in range(1, nx)]
    back = swap(back_sent.reshape(sources, SLOTS, 128), ("z", "c")).reshape(slots, 128)
    grad_gate, grad_up, grad_down, down_norms = call(
        grads_body,
        [((hid, width), F32)] * 3 + [((1, hid), F32)],
        here,
        *grads,
        far=True,
        scratch=[pltpu.VMEM((nx, 3 * hid, quarter), BF16)],
    )
    grad_tokens, grad_route, gate_norms, up_norms = call(
        combine_body,
        [((feat, count), BF16), ((2, count), F32)] + [((width // 128, 128), F32)] * 2,
        here,
        back,
        positions,
        scales,
        *norms,
        far=True,
        scratch=[pltpu.VMEM((nx, quarter // 64, 128), F32)],
    )
    return (
        grad_tokens.T,
        grad_route.T,
        grad_gate[None],
        grad_up[None],
        grad_down[None],
        gate_norms.reshape(1, width),
        up_norms.reshape(1, width),
        down_norms,
    )


def solution(mesh):
    ep, tp = ("z", "c"), ("y", "x")
    fine = Mesh(mesh.devices.reshape(12, 2, 8, 4), ep + tp)
    in_specs = (
        P(ep, tp),
        P(ep, None),
        P(ep, None),
        P(ep, tp),
        P(ep, tp, None),
        P(ep, tp, None),
        P(ep, tp, None),
    )
    out_specs = (
        P(ep, tp),
        P(ep, None),
        P(ep, tp, None),
        P(ep, tp, None),
        P(ep, tp, None),
        P(ep, None),
        P(ep, None),
        P(ep, tp),
    )
    return jax.shard_map(layer, mesh=fine, in_specs=in_specs, out_specs=out_specs, check_vma=False)
```
